32 devices in a mesh: grp: 2 (over y), sp: 8 (over z, core), tp: 2 (over x).
Axes of the slice: x: 2, y: 2, z: 4, core: 2. Of those that a mesh axis runs over, the one named last changes fastest.
Arguments:
- queries: bfloat16 [12288, 1024], P(('grp', 'sp'), 'tp'), parts along dimension 0, may hold values from -200 to 200
- key_rows: bfloat16 [12288, 512], P(('grp', 'sp'), 'tp'), parts along dimension 0, may hold values from -6 to 6
- value_rows: bfloat16 [12288, 512], P(('grp', 'sp'), 'tp'), parts along dimension 0, may hold values from -6 to 6
- doc_ids: int32 [12288], P(('grp', 'sp')), parts along dimension 0, may hold values from 0 to 3, never falling along the last dimension, each value on 1 to 3072 neighbouring positions
- sink_logits: float32 [16], P('tp'), may hold values from 2 to 7
- out_weight: bfloat16 [1024, 2048], P('tp', 'sp'), may hold values from -0.1875 to 0.1875
- residual: bfloat16 [12288, 2048], P(('grp', 'sp', 'tp')), parts along dimension 0, may hold values from -6 to 6
- gain_mixed: float32 [2048], replicated, may hold values from 0.1 to 1.9
- gain_before: float32 [2048], replicated, may hold values from 0.1 to 1.9
- gain_after: float32 [2048], replicated, may hold values from 0.1 to 1.9
- gate_weight: bfloat16 [2048, 6144], P('sp', 'tp'), may hold values from -0.125 to 0.125
- up_weight: bfloat16 [2048, 6144], P('sp', 'tp'), may hold values from -0.125 to 0.125
- down_weight: bfloat16 [6144, 2048], P('tp', 'sp'), may hold values from -0.078125 to 0.078125
Outputs:
- layer_out: bfloat16 [12288, 2048], P(('grp', 'sp', 'tp')), parts along dimension 0
The draws below stay inside these ranges and needn't reach their ends.
There are 2 independent parts, one for each index of `grp`. The reference program is written for one: setup_inputs(seed, part) draws one part's arguments, and reference() takes and returns one part's arrays. A program takes and returns all parts, laid end to end along the dimension named above; an argument that names none is the same for every part. Nothing has to cross between parts.
All inputs are finite; a program needn't handle non-finite values.
Results may differ from the reference program's by a relative error of at most 0.015.
Values may be sent and summed in bfloat16 or wider, within the bound.
A program may use at most 128 MiB of HBM per device.

```python
import math
import jax
import jax.numpy as jnp
import numpy as np
from jax import lax

D = 2048
HEADS = 16
KV_HEADS = 8
HEAD_DIM = 64
FF = 6144
WINDOW = 128
TOKENS = 6144
DOCS = 4
DOC_MOST = 3072
N_TP = 2


def drawn(key):
    base_keys = jnp.clip(jax.random.normal(jax.random.fold_in(key, 11), (TOKENS, KV_HEADS * HEAD_DIM), jnp.float32), -5.0, 5.0)
    base_queries = jnp.clip(jax.random.normal(jax.random.fold_in(key, 12), (TOKENS, HEADS * HEAD_DIM), jnp.float32), -5.0, 5.0)
    return (base_queries, base_keys)


def draw_queries(key, part):
    return drawn(key)[0].astype(jnp.bfloat16)


def draw_key_rows(key, part):
    return drawn(key)[1].astype(jnp.bfloat16)


def shard_levels(key, dims, pieces, smallest, top_value):
    level, own = 1.0, jax.random.fold_in(key, 6)
    for axis_at, blocks in pieces:
        heights = jnp.exp(jax.random.uniform(jax.random.fold_in(own, axis_at), (blocks,), jnp.float32, smallest / len(pieces), top_value / len(pieces)))
        level = level * jnp.repeat(heights, dims[axis_at] // blocks).reshape([-1 if axis == axis_at else 1 for axis in range(len(dims))])
    return level


def length_profile(amount, total, bound, skew):
    weights = [(1 << 20) // math.isqrt(rank ** skew) + 1 for rank in range(2, amount + 1)]
    spare, holding = total - bound - (amount - 1), [1] * (amount - 1)
    while spare > 0:
        candidates = [i for i in range(amount - 1) if holding[i] < bound]
        mass, remaining = sum([weights[i] for i in candidates]), spare
        for i in candidates:
            more = min(bound - holding[i], max(1, remaining * weights[i] // mass), spare)
            holding[i] = holding[i] + more
            spare = spare - more
    return np.array([bound] + holding)


def uneven_parts(stream_key, count, total, bound, skew):
    if count == 2:
        one = jax.random.randint(stream_key, (), max(1, total - bound), min(bound, total - 1) + 1)
        return jnp.stack([one, total - one])
    lengths = jnp.asarray(length_profile(count, total, bound, skew), jnp.int32)
    twos = (count - 1) // 2
    source_of, taker = lengths[1:1 + 2 * twos:2], lengths[2:2 + 2 * twos:2]
    margin = jnp.minimum(source_of - 1, bound - taker)
    moved = jax.random.randint(jax.random.fold_in(stream_key, 1), (twos,), 0, 1 << 20) % (margin + 1)
    lengths = lengths.at[1:1 + 2 * twos:2].set(source_of - moved).at[2:2 + 2 * twos:2].set(taker + moved)
    return lengths[jax.random.permutation(jax.random.fold_in(stream_key, 2), count)]


def centred(stream_key, dims, width, most, split=(), kind=jnp.bfloat16):
    level = shard_levels(stream_key, dims, split, -0.22, 0.18) if split else 1.0
    drawn = jax.random.normal(stream_key, dims, jnp.float32) * width * level
    return jnp.minimum(jnp.maximum(drawn, -most), most).astype(kind)


def setup_inputs(seed: int = 0, part: int = 0) -> dict:
    arg_keys = jax.random.split(jax.random.key(seed), 14)
    own_keys = jax.random.split(jax.random.fold_in(arg_keys[13], part), 14)
    return {
        "queries": draw_queries(jax.random.fold_in(jax.random.fold_in(arg_keys[13], part), 71), part),
        "key_rows": draw_key_rows(jax.random.fold_in(jax.random.fold_in(arg_keys[13], part), 71), part),
        "value_rows": centred(own_keys[2], (TOKENS, KV_HEADS * HEAD_DIM), 1.0, 6.0, ((0, 8), (1, 2))),
        "doc_ids": jnp.searchsorted(jnp.cumsum(uneven_parts(own_keys[3], DOCS, TOKENS, DOC_MOST, 1)), jnp.arange(TOKENS), side="right").astype(jnp.int32),
        "sink_logits": jnp.clip(2.0 + 5.0 * jax.random.uniform(arg_keys[4], (HEADS,), jnp.float32) ** shard_levels(arg_keys[4], (HEADS,), ((0, 2),), -0.2, 0.2), 2.0, 7.0),
        "out_weight": centred(arg_keys[5], (HEADS * HEAD_DIM, D), (HEADS * HEAD_DIM) ** -0.5, 0.1875, ((0, 2), (1, 8))),
        "residual": centred(own_keys[6], (TOKENS, D), 1.0, 6.0, ((0, 16),)),
        "gain_mixed": jnp.clip(1.0 + 0.18 * jax.random.normal(arg_keys[7], (D,), jnp.float32), 0.1, 1.9),
        "gain_before": jnp.clip(1.0 + 0.18 * jax.random.normal(arg_keys[8], (D,), jnp.float32), 0.1, 1.9),
        "gain_after": jnp.clip(1.0 + 0.18 * jax.random.normal(arg_keys[9], (D,), jnp.float32), 0.1, 1.9),
        "gate_weight": centred(arg_keys[10], (D, FF), D ** -0.5, 0.125, ((0, 8), (1, 2))),
        "up_weight": centred(arg_keys[11], (D, FF), D ** -0.5, 0.125, ((0, 8), (1, 2))),
        "down_weight": centred(arg_keys[12], (FF, D), FF ** -0.5, 0.078125, ((0, 2), (1, 8))),
    }


epsilon = 1e-06
masked_value = -1e+30

def stored(value):
    return lax.optimization_barrier(value.astype(jnp.bfloat16)).astype(jnp.float32)

def rms_scaled(value, gain):
    return value * lax.rsqrt(lax.optimization_barrier(jnp.mean(value * value, axis=-1, keepdims=True)) + epsilon) * gain

def reference(queries, key_rows, value_rows, doc_ids, sink_logits, out_weight, residual, gain_mixed, gain_before, gain_after, gate_weight, up_weight, down_weight):
    total = queries.shape[0]
    blocks = total // WINDOW
    group_size = HEADS // KV_HEADS
    padded_keys = jnp.concatenate([jnp.zeros((WINDOW, KV_HEADS * HEAD_DIM), jnp.bfloat16), key_rows], axis=0)
    padded_values = jnp.concatenate([jnp.zeros((WINDOW, KV_HEADS * HEAD_DIM), jnp.bfloat16), value_rows], axis=0)
    padded_docs = jnp.concatenate([jnp.zeros((WINDOW,), jnp.int32) - 1, doc_ids], axis=0)
    key_pos = jnp.arange(total + WINDOW, dtype=jnp.int32) - WINDOW

    def windows(array):
        first = array[:-WINDOW].reshape((blocks, WINDOW) + array.shape[1:])
        second = array[WINDOW:].reshape((blocks, WINDOW) + array.shape[1:])
        return jnp.concatenate([first, second], axis=1)
    key_blocks = windows(padded_keys).reshape(blocks, 2 * WINDOW, KV_HEADS, HEAD_DIM).astype(jnp.float32)
    value_blocks = windows(padded_values).reshape(blocks, 2 * WINDOW, KV_HEADS, HEAD_DIM).astype(jnp.float32)
    key_docs = windows(padded_docs)
    key_places = windows(key_pos)
    query_blocks = queries.reshape(blocks, WINDOW, KV_HEADS, group_size, HEAD_DIM).astype(jnp.float32)
    query_places = jnp.arange(total, dtype=jnp.int32).reshape(blocks, WINDOW)
    query_docs = doc_ids.reshape(blocks, WINDOW)
    scores = jnp.einsum('bqhgd,bkhd->bhgqk', query_blocks, key_blocks) * HEAD_DIM ** (-0.5)
    distance = query_places[:, :, None] - key_places[:, None, :]
    valid = (distance >= 0) & (distance < WINDOW) & (key_places[:, None, :] >= 0)
    valid = valid & (query_docs[:, :, None] == key_docs[:, None, :])
    scores = jnp.where(valid[:, None, None], scores, masked_value)
    sinks = sink_logits.reshape(KV_HEADS, group_size)[None, :, :, None]
    top = jnp.maximum(lax.optimization_barrier(jnp.max(scores, axis=-1)), sinks)
    weight = jnp.exp(scores - top[..., None])
    denom = lax.optimization_barrier(jnp.sum(weight, axis=-1)) + jnp.exp(sinks - top)
    weight_b = weight.astype(jnp.bfloat16).astype(jnp.float32)
    summed = jnp.einsum('bhgqk,bkhd->bqhgd', weight_b, value_blocks)
    scale = jnp.transpose(denom, (0, 3, 1, 2))[..., None]
    mixed = (summed / scale).reshape(total, HEADS * HEAD_DIM).astype(jnp.bfloat16)
    projected = stored(jnp.dot(mixed, out_weight, preferred_element_type=jnp.float32))
    after = stored(residual.astype(jnp.float32) + rms_scaled(projected, gain_mixed))
    normed = rms_scaled(after, gain_before).astype(jnp.bfloat16)
    gate = jnp.dot(normed, gate_weight, preferred_element_type=jnp.float32)
    upward = jnp.dot(normed, up_weight, preferred_element_type=jnp.float32)
    hidden = (jax.nn.silu(gate) * upward).astype(jnp.bfloat16)
    block_size = FF // N_TP
    summed_out = jnp.zeros((total, D), jnp.float32)
    for index in range(N_TP):
        partial_sum = jnp.dot(hidden[:, index * block_size:(index + 1) * block_size], down_weight[index * block_size:(index + 1) * block_size], preferred_element_type=jnp.float32)
        summed_out = summed_out + stored(partial_sum)
    ffn_out = stored(summed_out)
    return (after + 0.5 * rms_scaled(ffn_out, gain_after)).astype(jnp.bfloat16)
```

```python
import functools

import jax
import jax.numpy as jnp
from jax import lax
from jax.experimental import pallas as pl
from jax.experimental.pallas import tpu as pltpu
from jax.sharding import PartitionSpec as P

HEAD_DIM = 64
WINDOW = 128


epsilon = 1e-06
masked_value = -1e30


def passed_along(value, axis, steps):
    count = lax.axis_size(axis)
    first, last = (max(0, -steps), min(count, count - steps))
    return lax.ppermute(value, axis, [(source, source + steps) for source in range(first, last)])


def stored(value):
    return lax.optimization_barrier(value.astype(jnp.bfloat16)).astype(jnp.float32)


def rms_scaled(value, gain):
    return value * lax.rsqrt(jnp.mean(value * value, axis=-1, keepdims=True) + epsilon) * gain


def windows(array, blocks):
    first = array[:-WINDOW].reshape((blocks, WINDOW) + array.shape[1:])
    second = array[WINDOW:].reshape((blocks, WINDOW) + array.shape[1:])
    return jnp.concatenate([first, second], axis=1)


def attend(queries, key_rows, value_rows, doc_ids, sink_logits):
    length = queries.shape[0]
    blocks = length // WINDOW
    local_kv = key_rows.shape[1] // HEAD_DIM
    group_size = queries.shape[1] // HEAD_DIM // local_kv
    offset = lax.axis_index("sp") * length
    tail_keys, tail_values, tail_docs = passed_along(
        (key_rows[length - WINDOW :], value_rows[length - WINDOW :], doc_ids[length - WINDOW :]),
        "sp",
        1,
    )
    key_blocks = windows(jnp.concatenate([tail_keys, key_rows], axis=0), blocks).reshape(
        blocks, 2 * WINDOW, local_kv, HEAD_DIM
    )
    value_blocks = windows(jnp.concatenate([tail_values, value_rows], axis=0), blocks).reshape(
        blocks, 2 * WINDOW, local_kv, HEAD_DIM
    )
    key_docs = windows(jnp.concatenate([tail_docs, doc_ids], axis=0), blocks)
    key_places = windows(offset - WINDOW + jnp.arange(length + WINDOW, dtype=jnp.int32), blocks)
    query_places = (offset + jnp.arange(length, dtype=jnp.int32)).reshape(blocks, WINDOW)
    query_docs = doc_ids.reshape(blocks, WINDOW)
    query_blocks = queries.reshape(blocks, WINDOW, local_kv, group_size, HEAD_DIM)
    scores = jnp.einsum(
        "bqhgd,bkhd->bhgqk", query_blocks, key_blocks, preferred_element_type=jnp.float32
    ) * HEAD_DIM ** (-0.5)
    distance = query_places[:, :, None] - key_places[:, None, :]
    valid = (distance >= 0) & (distance < WINDOW) & (key_places[:, None, :] >= 0)
    valid = valid & (query_docs[:, :, None] == key_docs[:, None, :])
    scores = jnp.where(valid[:, None, None], scores, masked_value)
    sinks = sink_logits.reshape(local_kv, group_size)[None, :, :, None]
    top = jnp.maximum(jnp.max(scores, axis=-1), sinks)
    weight = jnp.exp(scores - top[..., None])
    denom = jnp.sum(weight, axis=-1) + jnp.exp(sinks - top)
    summed = jnp.einsum(
        "bhgqk,bkhd->bqhgd",
        weight.astype(jnp.bfloat16),
        value_blocks,
        preferred_element_type=jnp.float32,
    )
    scale = jnp.transpose(denom, (0, 3, 1, 2))[..., None]
    return (summed / scale).reshape(length, queries.shape[1]).astype(jnp.bfloat16)

MESH = pl.DeviceIdType.MESH
QUARTERS = 4
SPLIT = 2
LAG = 2
TILE = 256
STEP_ROWS = 32


def block_kernel(
    levels, queries, keys, values, docs, sinks, wout, resid, gain_m, gain_b, gain_a, gate, up, down, out,
    full_out, full_gu, full_down, q_buf, k_buf, v_buf, d_buf, mixed, after, normed, hidden, fsend, frecv, fown,
    local_sem, halo_send, halo_recv, o_send, o_recv, oy_send, oy_recv, oc_send, oc_recv,
    z_recv, z_up, z_dn, y_send, y_recv, c_send, c_recv, x_send, x_recv, f_send, f_recv, out_sem,
):
    y, s, x = lax.axis_index("grp"), lax.axis_index("sp"), lax.axis_index("tp")
    z, c = s // 2, s % 2
    count = 2 * levels
    y_peer, x_peer, c_peer = {"grp": 1 - y}, {"tp": 1 - x}, {"sp": z * 2 + 1 - c}
    above, below = {"sp": jnp.minimum(s + 2, count - 1)}, {"sp": jnp.maximum(s - 2, 0)}
    ahead, behind = {"sp": jnp.minimum(s + 1, count - 1)}, {"sp": jnp.maximum(s - 1, 0)}
    rows, dim, hid = q_buf.shape[0], full_gu.shape[1], full_gu.shape[2]
    mine = after.shape[0]
    blocks = rows // WINDOW
    kv_tiles = k_buf.shape[1] // (2 * HEAD_DIM)
    shard = gate.shape[0]
    half_rows = shard // 2
    out_rows = wout.shape[0] // 2
    out_cols = wout.shape[1]
    down_rows = down.shape[0] // 2
    width = down.shape[1] // 2
    quarter = hid // QUARTERS
    part_rows = down_rows // SPLIT
    chunks, pieces = 2 * QUARTERS, 2 * SPLIT
    own_rows, peer_rows = pl.ds(pl.multiple_of(x * mine, mine), mine), pl.ds(pl.multiple_of((1 - x) * mine, mine), mine)

    barrier = pltpu.get_barrier_semaphore()

    def greet(device):
        pl.semaphore_signal(barrier, inc=1, device_id=device, device_id_type=MESH)

    greet(y_peer)
    greet(x_peer)
    greet(c_peer)

    def greet_line(zz, _):
        @pl.when(zz != z)
        def _():
            greet({"sp": zz * 2 + c})

        return 0

    lax.fori_loop(0, levels, greet_line, 0)

    @pl.when((c == 1) & (z < levels - 1))
    def _():
        greet(ahead)

    @pl.when((c == 0) & (z > 0))
    def _():
        greet(behind)

    def local(source, target, n):
        return pltpu.make_async_copy(source, target, local_sem.at[n])

    shard_rows = pl.ds(pl.multiple_of(s * shard, shard), shard)
    loads = [
        local(wout, full_out.at[:, pl.ds(pl.multiple_of(s * out_cols, out_cols), out_cols)], 0),
        local(keys, k_buf.at[pl.ds(WINDOW, rows), :], 1),
        local(values, v_buf.at[pl.ds(WINDOW, rows), :], 2),
        local(docs, d_buf.at[pl.ds(1, blocks)], 3),
        local(queries, q_buf, 4),
        local(gate, full_gu.at[0, shard_rows, :], 5),
        local(up, full_gu.at[1, shard_rows, :], 6),
        local(down.at[:, pl.ds(0, width)], full_down.at[0, z, :, pl.ds(pl.multiple_of(c * width, width), width)], 7),
        local(down.at[:, pl.ds(width, width)], full_down.at[1, z, :, pl.ds(pl.multiple_of(c * width, width), width)], 8),
        local(resid, after, 9),
    ]
    for load in loads:
        load.start()

    links = jnp.where((c == 1) & (z < levels - 1), 1, 0) + jnp.where((c == 0) & (z > 0), 1, 0)
    pl.semaphore_wait(barrier, 3 + levels - 1 + links)

    def remote(source, target, send, recv, device):
        return pltpu.make_async_remote_copy(
            src_ref=source, dst_ref=target, send_sem=send, recv_sem=recv, device_id=device, device_id_type=MESH
        )

    def halo(n):
        source, target = (
            (keys.at[pl.ds(rows - WINDOW, WINDOW), :], k_buf.at[pl.ds(0, WINDOW), :]),
            (values.at[pl.ds(rows - WINDOW, WINDOW), :], v_buf.at[pl.ds(0, WINDOW), :]),
            (docs.at[pl.ds(blocks - 1, 1)], d_buf.at[pl.ds(0, 1)]),
        )[n]
        return remote(source, target, halo_send.at[n], halo_recv.at[n], ahead)

    @pl.when(s < count - 1)
    def _():
        for n in range(3):
            halo(n).start()

    def out_place(zz, cc, hh):
        column = pl.multiple_of((zz * 2 + cc) * out_cols, out_cols)
        return full_out.at[pl.ds(pl.multiple_of(hh * out_rows, out_rows), out_rows), pl.ds(column, out_cols)]

    def out_line(target, source):
        block = out_place(source, c, y)
        return remote(block, block, o_send.at[target], o_recv.at[source], {"sp": target * 2 + c})

    def out_across(zz, hh):
        block = out_place(zz, c, hh)
        return remote(block, block, oy_send.at[zz], oy_recv.at[zz], y_peer)

    def out_beside(zz, hh, cc):
        block = out_place(zz, cc, hh)
        return remote(block, block, oc_send.at[zz, hh], oc_recv.at[zz, hh], c_peer)

    def others(act):
        def one(zz, _):
            @pl.when(zz != z)
            def _():
                act(zz)

            return 0

        lax.fori_loop(0, levels, one, 0)

    def place(n, zz, cc, hh):
        stage, p = n
        if stage == 0:
            row = pl.multiple_of(((zz * 2 + cc) * 2 + hh) * half_rows, half_rows)
            column = pl.multiple_of((p // 2) * quarter, quarter)
            return full_gu.at[p % 2, pl.ds(row, half_rows), pl.ds(column, quarter)]
        row = pl.multiple_of(hh * down_rows + (p % SPLIT) * part_rows, part_rows)
        return full_down.at[p // SPLIT, zz, pl.ds(row, part_rows), pl.ds(pl.multiple_of(cc * width, width), width)]

    def at(n):
        return n[1] + chunks * n[0]

    def upward(n, zz):
        block = place(n, zz, c, y)
        return remote(block, block, z_up.at[at(n), zz], z_recv.at[at(n), zz], above)

    def downward(n, zz):
        block = place(n, zz, c, y)
        return remote(block, block, z_dn.at[at(n), zz], z_recv.at[at(n), zz], below)

    def across(n, zz, hh):
        block = place(n, zz, c, hh)
        return remote(block, block, y_send.at[at(n), zz], y_recv.at[at(n), zz], y_peer)

    def beside(n, zz, hh, cc):
        block = place(n, zz, cc, hh)
        return remote(block, block, c_send.at[at(n), zz, hh], c_recv.at[at(n), zz, hh], c_peer)

    def own(stage, amount):
        def one(p, _):
            n = (stage, p)

            @pl.when(z < levels - 1)
            def _():
                upward(n, z).start()

            @pl.when(z > 0)
            def _():
                downward(n, z).start()

            for hh in range(2):
                beside(n, z, hh, c).start()
            return 0

        lax.fori_loop(0, amount, one, 0)

    def from_line(n, t):
        low, high = z - t, z + t

        @pl.when(low >= 0)
        def _():
            upward(n, low).wait_recv()

            @pl.when(z < levels - 1)
            def _():
                upward(n, low).start()

            across(n, low, y).start()
            beside(n, low, y, c).start()

        @pl.when(high < levels)
        def _():
            downward(n, high).wait_recv()

            @pl.when(z > 0)
            def _():
                downward(n, high).start()

            across(n, high, y).start()
            beside(n, high, y, c).start()

    def from_side(n, t):
        for zz, there in ((z - t, z - t >= 0), (z + t, z + t < levels)):

            @pl.when(there)
            def _(zz=zz):
                across(n, zz, 1 - y).wait_recv()
                beside(n, zz, 1 - y, c).start()

    def from_partner(n, zz):
        for hh in range(2):
            beside(n, zz, hh, 1 - c).wait_recv()

    low_lane = lax.broadcasted_iota(jnp.int32, (1, 2 * HEAD_DIM), 1) < HEAD_DIM

    def attention(b, _):
        here = pl.ds(pl.multiple_of(b * WINDOW, WINDOW), WINDOW)
        span = pl.ds(pl.multiple_of(b * WINDOW, WINDOW), 2 * WINDOW)
        key_docs = jnp.concatenate([d_buf[b], d_buf[b + 1]], axis=1)
        query_docs = jnp.transpose(jnp.broadcast_to(d_buf[b + 1], (WINDOW, WINDOW)))
        query_docs = jnp.concatenate([query_docs, query_docs], axis=1)
        query_at = lax.broadcasted_iota(jnp.int32, (WINDOW, 2 * WINDOW), 0)
        key_at = lax.broadcasted_iota(jnp.int32, (WINDOW, 2 * WINDOW), 1)
        valid = (key_at > query_at) & (key_at <= query_at + WINDOW) & (query_docs == key_docs)
        for m in range(kv_tiles):
            lanes = slice(m * 2 * HEAD_DIM, (m + 1) * 2 * HEAD_DIM)
            key_tile = k_buf[span, lanes].astype(jnp.float32)
            value_tile = v_buf[span, lanes].astype(jnp.float32)
            key_turned = pltpu.roll(key_tile, HEAD_DIM, 1)
            value_turned = pltpu.roll(value_tile, HEAD_DIM, 1)
            for e in range(2):
                head = 2 * m + e
                first, second = (key_tile, key_turned) if e == 0 else (key_turned, key_tile)
                key_pair = jnp.where(low_lane, first, second).astype(jnp.bfloat16)
                first, second = (value_tile, value_turned) if e == 0 else (value_turned, value_tile)
                value_pair = jnp.where(low_lane, first, second).astype(jnp.bfloat16)
                columns = slice(head * 2 * HEAD_DIM, (head + 1) * 2 * HEAD_DIM)
                query = q_buf[here, columns].astype(jnp.float32) * HEAD_DIM ** (-0.5)
                stacked = jnp.concatenate(
                    [jnp.where(low_lane, query, 0.0), jnp.where(low_lane, 0.0, query)], axis=0
                ).astype(jnp.bfloat16)
                scores = lax.dot_general(
                    stacked, key_pair, (((1,), (1,)), ((), ())), preferred_element_type=jnp.float32
                )
                results = []
                for g in range(2):
                    sink = sinks[2 * head + g]
                    score = jnp.where(valid, scores[g * WINDOW : (g + 1) * WINDOW], masked_value)
                    top = jnp.maximum(jnp.max(score, axis=1, keepdims=True), sink)
                    weight = jnp.exp(score - top)
                    denom = jnp.sum(weight, axis=1, keepdims=True) + jnp.exp(sink - top)
                    summed = jnp.dot(weight.astype(jnp.bfloat16), value_pair, preferred_element_type=jnp.float32)
                    results.append(summed / denom)
                mixed[here, columns] = jnp.where(low_lane, results[0], results[1]).astype(jnp.bfloat16)
        return 0

    def project():
        def tile(j, _):
            cols = pl.ds(pl.multiple_of(j * TILE, TILE), TILE)
            fsend[j] = jnp.dot(mixed[peer_rows, :], full_out[:, cols], preferred_element_type=jnp.float32).astype(jnp.bfloat16)
            fown[j] = jnp.dot(mixed[own_rows, :], full_out[:, cols], preferred_element_type=jnp.float32).astype(jnp.bfloat16)
            return 0

        lax.fori_loop(0, dim // TILE, tile, 0)

    def sent_projection():
        return remote(fsend, frecv, x_send.at[0], x_recv.at[0], x_peer)

    def sent_normed(where):
        return remote(normed.at[where, :], normed.at[where, :], x_send.at[1], x_recv.at[1], x_peer)

    def norms():
        def tile(i, _):
            here = pl.ds(pl.multiple_of(i * STEP_ROWS, STEP_ROWS), STEP_ROWS)
            parts = [fown[j, here, :].astype(jnp.float32) + frecv[j, here, :].astype(jnp.float32) for j in range(dim // TILE)]
            projected = jnp.concatenate(parts, axis=1).astype(jnp.bfloat16).astype(jnp.float32)
            total = (after[here, :].astype(jnp.float32) + rms_scaled(projected, gain_m[...])).astype(jnp.bfloat16)
            after[here, :] = total
            placed = pl.ds(pl.multiple_of(x * mine + i * STEP_ROWS, STEP_ROWS), STEP_ROWS)
            normed[placed, :] = rms_scaled(total.astype(jnp.float32), gain_b[...]).astype(jnp.bfloat16)
            return 0

        lax.fori_loop(0, mine // STEP_ROWS, tile, 0)

    def hidden_tile(j, _):
        cols = pl.ds(pl.multiple_of(j * TILE, TILE), TILE)
        g = jnp.dot(normed[...], full_gu[0, :, cols], preferred_element_type=jnp.float32)
        u = jnp.dot(normed[...], full_gu[1, :, cols], preferred_element_type=jnp.float32)
        hidden[:, cols] = (g / (1.0 + jnp.exp(-g)) * u).astype(jnp.bfloat16)
        return 0

    per_quarter = quarter // TILE

    def tiles_after(g):
        return jnp.where(g % 2 == 1, per_quarter * (g // 2) + (per_quarter + 1) // 2, per_quarter * (g // 2))

    def filled(g):
        def one(zz, _):
            from_partner((0, g), zz)
            return 0

        lax.fori_loop(0, levels, one, 0)

    def sent_sum(n):
        return remote(fsend.at[n], frecv.at[n], f_send.at[n], f_recv.at[n], x_peer)

    def lowered(k, zz):
        for r in range(SPLIT):
            from_partner((1, k * SPLIT + r), zz)
        n = k * levels + zz
        block = full_down.at[k, zz]
        fsend[n] = jnp.dot(hidden[peer_rows, :], block[...], preferred_element_type=jnp.float32).astype(jnp.bfloat16)
        sent_sum(n).start()
        fown[n] = jnp.dot(hidden[own_rows, :], block[...], preferred_element_type=jnp.float32).astype(jnp.bfloat16)

    def ring(k, t):
        def one(side, _):
            zz = z - t + 2 * t * side

            @pl.when((zz >= 0) & (zz < levels))
            def _():
                lowered(k, zz)

            return 0

        lax.fori_loop(0, jnp.where(t == 0, 1, 2), one, 0)

    def side_before(p, t):
        @pl.when(p >= LAG)
        def _():
            from_side((0, p - LAG), t)

        if t > 1:

            @pl.when(p < LAG)
            def _():
                from_side((0, p - LAG + chunks), t - 1)

    def line_steps(t, first, last):
        def one(p, _):
            from_line((0, p), t)
            side_before(p, t)
            return 0

        lax.fori_loop(first, last, one, 0)

    loads[0].wait()
    others(lambda zz: out_line(zz, z).start())
    for hh in range(2):
        out_beside(z, hh, c).start()
    loads[5].wait()
    loads[6].wait()
    own(0, chunks)
    for n in range(1, 5):
        loads[n].wait()

    @pl.when(s == 0)
    def _():
        k_buf[pl.ds(0, WINDOW), :] = jnp.zeros((WINDOW, k_buf.shape[1]), k_buf.dtype)
        v_buf[pl.ds(0, WINDOW), :] = jnp.zeros((WINDOW, v_buf.shape[1]), v_buf.dtype)
        d_buf[0] = jnp.full((1, WINDOW), -1, jnp.int32)

    @pl.when(s > 0)
    def _():
        for n in range(3):
            halo(n).wait_recv()

    lax.fori_loop(0, blocks // 2, attention, 0)

    def out_arrived(zz):
        out_line(z, zz).wait_recv()
        out_across(zz, y).start()
        out_beside(zz, y, c).start()

    others(out_arrived)
    lax.fori_loop(blocks // 2, blocks, attention, 0)
    line_steps(1, 0, 1)

    def out_crossed(zz):
        out_across(zz, 1 - y).wait_recv()
        out_beside(zz, 1 - y, c).start()

    others(out_crossed)
    line_steps(1, 1, 2)

    def out_filled(zz, _):
        for hh in range(2):
            out_beside(zz, hh, 1 - c).wait_recv()
        return 0

    lax.fori_loop(0, levels, out_filled, 0)
    project()
    sent_projection().start()
    line_steps(1, 2, chunks)
    line_steps(2, 0, LAG + 1)
    loads[9].wait()
    sent_projection().wait()
    norms()
    sent_normed(own_rows).start()
    line_steps(2, LAG + 1, chunks)
    for t in range(3, levels - 1):
        line_steps(t, 0, chunks)
    loads[7].wait()
    loads[8].wait()
    own(1, pieces)
    last = levels - 1
    line_steps(last, 0, LAG + 1)
    sent_normed(own_rows).wait_send()
    sent_normed(peer_rows).wait_recv()
    filled(0)

    def gated(p, _):
        from_line((0, p), last)
        from_side((0, p - LAG), last)
        filled(p - LAG)
        lax.fori_loop(tiles_after(p - LAG - 1), tiles_after(p - LAG), hidden_tile, 0)
        return 0

    lax.fori_loop(LAG + 1, chunks, gated, 0)

    def closing(u, _):
        from_line((1, u), 1)
        g = u - LAG + chunks

        @pl.when(u < LAG)
        def _():
            from_side((0, g), last)
            filled(g)

        @pl.when(u >= LAG)
        def _():
            from_side((1, u - LAG), 1)

        done = jnp.where(u < LAG, tiles_after(g), jnp.where(u == LAG, hid // TILE, 0))
        begun = jnp.where(u < LAG, tiles_after(g - 1), jnp.where(u == LAG, tiles_after(chunks - 1), 0))
        lax.fori_loop(begun, done, hidden_tile, 0)
        return 0

    lax.fori_loop(0, pieces, closing, 0)
    lowered(0, z)
    flat = pieces * (levels - 1)

    def settled(v):
        @pl.when(v % SPLIT == SPLIT - 1)
        def _():
            ring((v % pieces) // SPLIT, v // pieces + 1)

    settled(jnp.int32(pieces - LAG - 1))

    def lowering(u, _):
        from_line((1, u % pieces), u // pieces + 1)
        v = u - LAG
        from_side((1, v % pieces), v // pieces + 1)

        @pl.when(u == pieces)
        def _():
            lowered(1, z)

        settled(v)
        return 0

    lax.fori_loop(pieces, flat, lowering, 0)

    def ending(v, _):
        from_side((1, v % pieces), v // pieces + 1)
        settled(v)
        return 0

    lax.fori_loop(flat - LAG, flat, ending, 0)

    @pl.when(s < count - 1)
    def _():
        for n in range(3):
            halo(n).wait_send()

    for hh in range(2):
        out_beside(z, hh, c).wait_send()

    def out_drained(zz):
        out_line(zz, z).wait_send()
        out_across(zz, y).wait_send()
        for hh in range(2):
            out_beside(zz, hh, c).wait_send()

    others(out_drained)

    def drain(zz, _):
        for stage, amount in ((0, chunks), (1, pieces)):

            def one(p, _, stage=stage):
                n = (stage, p)
                for hh in range(2):
                    beside(n, zz, hh, c).wait_send()

                @pl.when((zz <= z) & (z < levels - 1))
                def _():
                    upward(n, zz).wait_send()

                @pl.when((zz >= z) & (z > 0))
                def _():
                    downward(n, zz).wait_send()

                @pl.when(zz != z)
                def _():
                    across(n, zz, y).wait_send()

                return 0

            lax.fori_loop(0, amount, one, 0)
        return 0

    lax.fori_loop(0, levels, drain, 0)

    def sums(n, _):
        sent_sum(n).wait()
        return 0

    lax.fori_loop(0, 2 * levels, sums, 0)

    def finish(i, _):
        here = pl.ds(pl.multiple_of(i * STEP_ROWS, STEP_ROWS), STEP_ROWS)
        parts = [
            fown[k * levels + zz, here, cc * width : (cc + 1) * width].astype(jnp.float32)
            + frecv[k * levels + zz, here, cc * width : (cc + 1) * width].astype(jnp.float32)
            for zz in range(levels)
            for cc in range(2)
            for k in range(2)
        ]
        ffn_out = jnp.concatenate(parts, axis=1).astype(jnp.bfloat16).astype(jnp.float32)
        out[here, :] = (after[here, :].astype(jnp.float32) + 0.5 * rms_scaled(ffn_out, gain_a[...])).astype(jnp.bfloat16)
        return 0

    lax.fori_loop(0, mine // STEP_ROWS, finish, 0)


def fused(
    queries, key_rows, value_rows, doc_ids, sink_logits, out_weight,
    residual, gain_mixed, gain_before, gain_after, gate_weight, up_weight, down_weight,
):
    levels = lax.axis_size("sp") // 2
    rows, dim = queries.shape[0], residual.shape[1]
    blocks = rows // WINDOW
    mine = residual.shape[0]
    hid = gate_weight.shape[1]
    heads = out_weight.shape[0]
    half = down_weight.shape[1] // 2
    vmem, whole = pl.BlockSpec(memory_space=pltpu.VMEM), pl.BlockSpec(memory_space=pl.ANY)
    scalars = pl.BlockSpec(memory_space=pltpu.SMEM)
    bf16, dma = jnp.bfloat16, pltpu.SemaphoreType.DMA
    pieces = 2 * QUARTERS + 2 * SPLIT
    return pl.pallas_call(
        functools.partial(block_kernel, levels),
        out_shape=jax.ShapeDtypeStruct((mine, dim), bf16),
        in_specs=[whole] * 4 + [scalars] + [whole] * 2 + [vmem] * 3 + [whole] * 3,
        out_specs=vmem,
        scratch_shapes=[
            pltpu.VMEM((heads, dim), bf16),
            pltpu.VMEM((2, dim, hid), bf16),
            pltpu.VMEM((2, levels, hid, 2 * half), bf16),
            pltpu.VMEM(queries.shape, bf16),
            pltpu.VMEM((rows + WINDOW, key_rows.shape[1]), bf16),
            pltpu.VMEM((rows + WINDOW, value_rows.shape[1]), bf16),
            pltpu.VMEM((blocks + 1, 1, WINDOW), jnp.int32),
            pltpu.VMEM(queries.shape, bf16),
            pltpu.VMEM((mine, dim), bf16),
            pltpu.VMEM((rows, dim), bf16),
            pltpu.VMEM((rows, hid), bf16),
            pltpu.VMEM((2 * levels, mine, 2 * half), bf16),
            pltpu.VMEM((2 * levels, mine, 2 * half), bf16),
            pltpu.VMEM((2 * levels, mine, 2 * half), bf16),
            dma((10,)),
            dma((3,)),
            dma((3,)),
            dma((levels,)),
            dma((levels,)),
            dma((levels,)),
            dma((levels,)),
            dma((levels, 2)),
            dma((levels, 2)),
            dma((pieces, levels)),
            dma((pieces, levels)),
            dma((pieces, levels)),
            dma((pieces, levels)),
            dma((pieces, levels)),
            dma((pieces, levels, 2)),
            dma((pieces, levels, 2)),
            dma((2,)),
            dma((2,)),
            dma((2 * levels,)),
            dma((2 * levels,)),
            dma((1,)),
        ],
        compiler_params=pltpu.CompilerParams(collective_id=0, has_side_effects=True, vmem_limit_bytes=67043328),
    )(
        queries, key_rows, value_rows, doc_ids.reshape(blocks, 1, WINDOW), sink_logits, out_weight,
        residual, gain_mixed[None], gain_before[None], gain_after[None], gate_weight, up_weight, down_weight,
    )


def per_device(
    queries,
    key_rows,
    value_rows,
    doc_ids,
    sink_logits,
    out_weight,
    residual,
    gain_mixed,
    gain_before,
    gain_after,
    gate_weight,
    up_weight,
    down_weight,
):
    pairs = lax.axis_size("grp") == 2 and lax.axis_size("tp") == 2
    if pairs and lax.axis_size("sp") % 2 == 0 and lax.axis_size("sp") >= 8:
        return fused(
            queries, key_rows, value_rows, doc_ids, sink_logits, out_weight,
            residual, gain_mixed, gain_before, gain_after, gate_weight, up_weight, down_weight,
        )
    mixed = attend(queries, key_rows, value_rows, doc_ids, sink_logits)
    head_columns = lax.all_gather(out_weight, "sp", axis=1, tiled=True)
    projected = lax.psum_scatter(
        jnp.dot(mixed, head_columns, preferred_element_type=jnp.float32).astype(jnp.bfloat16),
        "tp",
        scatter_dimension=0,
        tiled=True,
    ).astype(jnp.float32)
    projected = stored(projected)
    after = stored(residual.astype(jnp.float32) + rms_scaled(projected, gain_mixed))
    normed = rms_scaled(after, gain_before).astype(jnp.bfloat16)
    full_gate, full_up, full_down = (
        lax.all_gather(gate_weight, "sp", axis=0, tiled=True),
        lax.all_gather(up_weight, "sp", axis=0, tiled=True),
        lax.all_gather(down_weight, "sp", axis=1, tiled=True),
    )
    piece = lax.all_gather(normed, "tp", axis=0, tiled=True)
    gate = jnp.dot(piece, full_gate, preferred_element_type=jnp.float32)
    upward = jnp.dot(piece, full_up, preferred_element_type=jnp.float32)
    hidden = (jax.nn.silu(gate) * upward).astype(jnp.bfloat16)
    ffn_out = stored(
        lax.psum_scatter(
            jnp.dot(hidden, full_down, preferred_element_type=jnp.float32).astype(jnp.bfloat16),
            "tp",
            scatter_dimension=0,
            tiled=True,
        ).astype(jnp.float32)
    )
    return (after + 0.5 * rms_scaled(ffn_out, gain_after)).astype(jnp.bfloat16)


def solution(mesh):
    return jax.shard_map(
        per_device,
        mesh=mesh,
        in_specs=(
            P(("grp", "sp"), "tp"),
            P(("grp", "sp"), "tp"),
            P(("grp", "sp"), "tp"),
            P(("grp", "sp")),
            P("tp"),
            P("tp", "sp"),
            P(("grp", "sp", "tp"), None),
            P(),
            P(),
            P(),
            P("sp", "tp"),
            P("sp", "tp"),
            P("tp", "sp"),
        ),
        out_specs=P(("grp", "sp", "tp"), None),
        check_vma=False,
    )
```

```python
import functools

import jax
import jax.numpy as jnp
from jax import lax
from jax.experimental import pallas as pl
from jax.experimental.pallas import tpu as pltpu
from jax.sharding import PartitionSpec as P

HEAD_DIM = 64
WINDOW = 128


epsilon = 1e-06
masked_value = -1e30


def passed_along(value, axis, steps):
    count = lax.axis_size(axis)
    first, last = (max(0, -steps), min(count, count - steps))
    return lax.ppermute(value, axis, [(source, source + steps) for source in range(first, last)])


def stored(value):
    return lax.optimization_barrier(value.astype(jnp.bfloat16)).astype(jnp.float32)


def rms_scaled(value, gain):
    return value * lax.rsqrt(jnp.mean(value * value, axis=-1, keepdims=True) + epsilon) * gain


def windows(array, blocks):
    first = array[:-WINDOW].reshape((blocks, WINDOW) + array.shape[1:])
    second = array[WINDOW:].reshape((blocks, WINDOW) + array.shape[1:])
    return jnp.concatenate([first, second], axis=1)


def attend(queries, key_rows, value_rows, doc_ids, sink_logits):
    length = queries.shape[0]
    blocks = length // WINDOW
    local_kv = key_rows.shape[1] // HEAD_DIM
    group_size = queries.shape[1] // HEAD_DIM // local_kv
    offset = lax.axis_index("sp") * length
    tail_keys, tail_values, tail_docs = passed_along(
        (key_rows[length - WINDOW :], value_rows[length - WINDOW :], doc_ids[length - WINDOW :]),
        "sp",
        1,
    )
    key_blocks = windows(jnp.concatenate([tail_keys, key_rows], axis=0), blocks).reshape(
        blocks, 2 * WINDOW, local_kv, HEAD_DIM
    )
    value_blocks = windows(jnp.concatenate([tail_values, value_rows], axis=0), blocks).reshape(
        blocks, 2 * WINDOW, local_kv, HEAD_DIM
    )
    key_docs = windows(jnp.concatenate([tail_docs, doc_ids], axis=0), blocks)
    key_places = windows(offset - WINDOW + jnp.arange(length + WINDOW, dtype=jnp.int32), blocks)
    query_places = (offset + jnp.arange(length, dtype=jnp.int32)).reshape(blocks, WINDOW)
    query_docs = doc_ids.reshape(blocks, WINDOW)
    query_blocks = queries.reshape(blocks, WINDOW, local_kv, group_size, HEAD_DIM)
    scores = jnp.einsum(
        "bqhgd,bkhd->bhgqk", query_blocks, key_blocks, preferred_element_type=jnp.float32
    ) * HEAD_DIM ** (-0.5)
    distance = query_places[:, :, None] - key_places[:, None, :]
    valid = (distance >= 0) & (distance < WINDOW) & (key_places[:, None, :] >= 0)
    valid = valid & (query_docs[:, :, None] == key_docs[:, None, :])
    scores = jnp.where(valid[:, None, None], scores, masked_value)
    sinks = sink_logits.reshape(local_kv, group_size)[None, :, :, None]
    top = jnp.maximum(jnp.max(scores, axis=-1), sinks)
    weight = jnp.exp(scores - top[..., None])
    denom = jnp.sum(weight, axis=-1) + jnp.exp(sinks - top)
    summed = jnp.einsum(
        "bhgqk,bkhd->bqhgd",
        weight.astype(jnp.bfloat16),
        value_blocks,
        preferred_element_type=jnp.float32,
    )
    scale = jnp.transpose(denom, (0, 3, 1, 2))[..., None]
    return (summed / scale).reshape(length, queries.shape[1]).astype(jnp.bfloat16)

MESH = pl.DeviceIdType.MESH
QUARTERS = 4
SPLIT = 2
LAG = 2
TILE = 256
STEP_ROWS = 32
FINAL_ROWS = 64
NORMS_AT = 11


def block_kernel(
    levels, queries, keys, values, docs, sinks, wout, resid, gain_m, gain_b, gain_a, gate, up, down, out,
    full_out, full_gu, full_down, q_buf, k_buf, v_buf, d_buf, mixed, after, normed, hidden, fsum, frecv,
    local_sem, halo_send, halo_recv, o_sent, o_recv, oy_recv, oc_recv,
    z_recv, z_up, z_dn, y_sent, y_recv, c_sent, c_recv, x_send, x_recv, f_sent, f_recv,
):
    y, s, x = lax.axis_index("grp"), lax.axis_index("sp"), lax.axis_index("tp")
    z, c = s // 2, s % 2
    count = 2 * levels
    y_peer, x_peer, c_peer = {"grp": 1 - y}, {"tp": 1 - x}, {"sp": z * 2 + 1 - c}
    above, below = {"sp": jnp.minimum(s + 2, count - 1)}, {"sp": jnp.maximum(s - 2, 0)}
    ahead, behind = {"sp": jnp.minimum(s + 1, count - 1)}, {"sp": jnp.maximum(s - 1, 0)}
    rows, dim, hid = q_buf.shape[0], full_gu.shape[1], full_gu.shape[2]
    mine = after.shape[0]
    blocks = rows // WINDOW
    kv_tiles = k_buf.shape[1] // (2 * HEAD_DIM)
    shard = gate.shape[0]
    half_rows = shard // 2
    out_rows = wout.shape[0] // 2
    out_cols = wout.shape[1]
    down_rows = down.shape[0] // 2
    width = down.shape[1] // 2
    quarter = hid // QUARTERS
    part_rows = down_rows // SPLIT
    chunks, pieces = 2 * QUARTERS, 2 * SPLIT
    own_rows, peer_rows = pl.ds(pl.multiple_of(x * mine, mine), mine), pl.ds(pl.multiple_of((1 - x) * mine, mine), mine)

    barrier = pltpu.get_barrier_semaphore()

    def greet(device):
        pl.semaphore_signal(barrier, inc=1, device_id=device, device_id_type=MESH)

    greet(y_peer)
    greet(x_peer)
    greet(c_peer)

    def greet_line(zz, _):
        @pl.when(zz != z)
        def _():
            greet({"sp": zz * 2 + c})

        return 0

    lax.fori_loop(0, levels, greet_line, 0)

    @pl.when((c == 1) & (z < levels - 1))
    def _():
        greet(ahead)

    @pl.when((c == 0) & (z > 0))
    def _():
        greet(behind)

    def local(source, target, n):
        return pltpu.make_async_copy(source, target, local_sem.at[n])

    shard_rows = pl.ds(pl.multiple_of(s * shard, shard), shard)
    loads = [
        local(wout, full_out.at[:, pl.ds(pl.multiple_of(s * out_cols, out_cols), out_cols)], 0),
        local(keys, k_buf.at[pl.ds(WINDOW, rows), :], 1),
        local(values, v_buf.at[pl.ds(WINDOW, rows), :], 2),
        local(docs, d_buf.at[:, pl.ds(WINDOW, rows)], 3),
        local(queries, q_buf, 4),
        local(gate, full_gu.at[0, shard_rows, :], 5),
        local(up, full_gu.at[1, shard_rows, :], 6),
        local(down.at[:, pl.ds(0, width)], full_down.at[0, z, :, pl.ds(pl.multiple_of(c * width, width), width)], 7),
        local(down.at[:, pl.ds(width, width)], full_down.at[1, z, :, pl.ds(pl.multiple_of(c * width, width), width)], 8),
        local(resid, after, 9),
    ]
    for load in loads:
        load.start()

    links = jnp.where((c == 1) & (z < levels - 1), 1, 0) + jnp.where((c == 0) & (z > 0), 1, 0)
    pl.semaphore_wait(barrier, 3 + levels - 1 + links)

    def remote(source, target, send, recv, device):
        return pltpu.make_async_remote_copy(
            src_ref=source, dst_ref=target, send_sem=send, recv_sem=recv, device_id=device, device_id_type=MESH
        )

    def halo(n):
        source, target = (
            (keys.at[pl.ds(rows - WINDOW, WINDOW), :], k_buf.at[pl.ds(0, WINDOW), :]),
            (values.at[pl.ds(rows - WINDOW, WINDOW), :], v_buf.at[pl.ds(0, WINDOW), :]),
            (docs.at[:, pl.ds(rows - WINDOW, WINDOW)], d_buf.at[:, pl.ds(0, WINDOW)]),
        )[n]
        return remote(source, target, halo_send.at[n], halo_recv.at[n], ahead)

    @pl.when(s < count - 1)
    def _():
        for n in range(3):
            halo(n).start()

    def out_place(zz, cc, hh):
        column = pl.multiple_of((zz * 2 + cc) * out_cols, out_cols)
        return full_out.at[pl.ds(pl.multiple_of(hh * out_rows, out_rows), out_rows), pl.ds(column, out_cols)]

    def out_line(target, source):
        block = out_place(source, c, y)
        return remote(block, block, o_sent.at[0], o_recv.at[source], {"sp": target * 2 + c})

    def out_across(zz, hh):
        block = out_place(zz, c, hh)
        return remote(block, block, o_sent.at[1], oy_recv.at[zz], y_peer)

    def out_beside(zz, hh, cc):
        block = out_place(zz, cc, hh)
        return remote(block, block, o_sent.at[2], oc_recv.at[0], c_peer)

    def others(act):
        def one(zz, _):
            @pl.when(zz != z)
            def _():
                act(zz)

            return 0

        lax.fori_loop(0, levels, one, 0)

    def place(n, zz, cc, hh):
        stage, p = n
        if stage == 0:
            row = pl.multiple_of(((zz * 2 + cc) * 2 + hh) * half_rows, half_rows)
            column = pl.multiple_of((p // 2) * quarter, quarter)
            return full_gu.at[p % 2, pl.ds(row, half_rows), pl.ds(column, quarter)]
        row = pl.multiple_of(hh * down_rows + (p % SPLIT) * part_rows, part_rows)
        return full_down.at[p // SPLIT, zz, pl.ds(row, part_rows), pl.ds(pl.multiple_of(cc * width, width), width)]

    def at(n):
        return n[1] + chunks * n[0]

    def upward(n, zz):
        block = place(n, zz, c, y)
        return remote(block, block, z_up.at[n[0], zz], z_recv.at[at(n), zz], above)

    def downward(n, zz):
        block = place(n, zz, c, y)
        return remote(block, block, z_dn.at[n[0], zz], z_recv.at[at(n), zz], below)

    def across(n, zz, hh):
        block = place(n, zz, c, hh)
        return remote(block, block, y_sent.at[n[0]], y_recv.at[at(n), zz], y_peer)

    def beside(n, zz, hh, cc):
        block = place(n, zz, cc, hh)
        group = n[1] if n[0] == 0 else chunks + n[1] // SPLIT * levels + zz
        return remote(block, block, c_sent.at[n[0]], c_recv.at[group], c_peer)

    def own(stage, amount):
        def one(p, _):
            n = (stage, p)

            @pl.when(z < levels - 1)
            def _():
                upward(n, z).start()

            @pl.when(z > 0)
            def _():
                downward(n, z).start()

            for hh in range(2):
                beside(n, z, hh, c).start()
            return 0

        lax.fori_loop(0, amount, one, 0)

    def from_line(n, t):
        low, high = z - t, z + t

        @pl.when(low >= 0)
        def _():
            upward(n, low).wait_recv()

            @pl.when(z < levels - 1)
            def _():
                upward(n, low).start()

            across(n, low, y).start()
            beside(n, low, y, c).start()

        @pl.when(high < levels)
        def _():
            downward(n, high).wait_recv()

            @pl.when(z > 0)
            def _():
                downward(n, high).start()

            across(n, high, y).start()
            beside(n, high, y, c).start()

    ends = jnp.minimum(z, levels - 1 - z)

    def side_at(i, amount):
        paired = i < 2 * ends * amount
        rest = i - 2 * ends * amount
        t = jnp.where(paired, i // (2 * amount) + 1, ends + 1 + rest // amount)
        p = jnp.where(paired, (i % (2 * amount)) // 2, rest % amount)
        upper = jnp.where(paired, i % 2 == 1, 2 * z < levels)
        return p, jnp.where(upper, z + t, z - t)

    def from_side(stage, i):
        p, zz = side_at(i, pieces if stage else chunks)
        n = (stage, p)
        across(n, zz, 1 - y).wait_recv()
        beside(n, zz, 1 - y, c).start()

    def line_step(stage, i):
        amount = pieces if stage else chunks
        from_line((stage, i % amount), i // amount + 1)

    def taken(block, semaphore):
        remote(block, block, semaphore, semaphore, c_peer).wait_recv()

    low_lane = lax.broadcasted_iota(jnp.int32, (1, 2 * HEAD_DIM), 1) < HEAD_DIM

    def attention(b, _):
        here = pl.ds(pl.multiple_of(b * WINDOW, WINDOW), WINDOW)
        span = pl.ds(pl.multiple_of(b * WINDOW, WINDOW), 2 * WINDOW)
        key_docs = d_buf[:, span]
        own_docs = d_buf[:, pl.ds(pl.multiple_of((b + 1) * WINDOW, WINDOW), WINDOW)]
        query_docs = jnp.transpose(jnp.broadcast_to(own_docs, (WINDOW, WINDOW)))
        query_docs = jnp.concatenate([query_docs, query_docs], axis=1)
        query_at = lax.broadcasted_iota(jnp.int32, (WINDOW, 2 * WINDOW), 0)
        key_at = lax.broadcasted_iota(jnp.int32, (WINDOW, 2 * WINDOW), 1)
        valid = (key_at > query_at) & (key_at <= query_at + WINDOW) & (query_docs == key_docs)
        for m in range(kv_tiles):
            lanes = slice(m * 2 * HEAD_DIM, (m + 1) * 2 * HEAD_DIM)
            key_tile = k_buf[span, lanes].astype(jnp.float32)
            value_tile = v_buf[span, lanes].astype(jnp.float32)
            key_turned = pltpu.roll(key_tile, HEAD_DIM, 1)
            value_turned = pltpu.roll(value_tile, HEAD_DIM, 1)
            for e in range(2):
                head = 2 * m + e
                first, second = (key_tile, key_turned) if e == 0 else (key_turned, key_tile)
                key_pair = jnp.where(low_lane, first, second).astype(jnp.bfloat16)
                first, second = (value_tile, value_turned) if e == 0 else (value_turned, value_tile)
                value_pair = jnp.where(low_lane, first, second).astype(jnp.bfloat16)
                columns = slice(head * 2 * HEAD_DIM, (head + 1) * 2 * HEAD_DIM)
                query = q_buf[here, columns].astype(jnp.float32) * HEAD_DIM ** (-0.5)
                stacked = jnp.concatenate(
                    [jnp.where(low_lane, query, 0.0), jnp.where(low_lane, 0.0, query)], axis=0
                ).astype(jnp.bfloat16)
                scores = lax.dot_general(
                    stacked, key_pair, (((1,), (1,)), ((), ())), preferred_element_type=jnp.float32
                )
                results = []
                for g in range(2):
                    sink = sinks[2 * head + g]
                    score = jnp.where(valid, scores[g * WINDOW : (g + 1) * WINDOW], masked_value)
                    top = jnp.maximum(jnp.max(score, axis=1, keepdims=True), sink)
                    weight = jnp.exp(score - top)
                    denom = jnp.sum(weight, axis=1, keepdims=True) + jnp.exp(sink - top)
                    summed = jnp.dot(weight.astype(jnp.bfloat16), value_pair, preferred_element_type=jnp.float32)
                    results.append(summed / denom)
                mixed[here, columns] = jnp.where(low_lane, results[0], results[1]).astype(jnp.bfloat16)
        return 0

    def project():
        def tile(j, _):
            cols = pl.ds(pl.multiple_of(j * TILE, TILE), TILE)
            fsum[j] = jnp.dot(mixed[...], full_out[:, cols], preferred_element_type=jnp.float32).astype(jnp.bfloat16)
            return 0

        lax.fori_loop(0, dim // TILE, tile, 0)

    def sent_projection():
        return remote(fsum.at[:, peer_rows, :], frecv, x_send.at[0], x_recv.at[0], x_peer)

    def sent_normed(where):
        return remote(normed.at[where, :], normed.at[where, :], x_send.at[1], x_recv.at[1], x_peer)

    def norms():
        def tile(i, _):
            here = pl.ds(pl.multiple_of(i * STEP_ROWS, STEP_ROWS), STEP_ROWS)
            placed = pl.ds(pl.multiple_of(x * mine + i * STEP_ROWS, STEP_ROWS), STEP_ROWS)
            parts = [fsum[j, placed, :].astype(jnp.float32) + frecv[j, here, :].astype(jnp.float32) for j in range(dim // TILE)]
            projected = jnp.concatenate(parts, axis=1).astype(jnp.bfloat16).astype(jnp.float32)
            total = (after[here, :].astype(jnp.float32) + rms_scaled(projected, gain_m[...])).astype(jnp.bfloat16)
            after[here, :] = total
            normed[placed, :] = rms_scaled(total.astype(jnp.float32), gain_b[...]).astype(jnp.bfloat16)
            return 0

        lax.fori_loop(0, mine // STEP_ROWS, tile, 0)

    def hidden_tile(j, _):
        cols = pl.ds(pl.multiple_of(j * TILE, TILE), TILE)
        g = jnp.dot(normed[...], full_gu[0, :, cols], preferred_element_type=jnp.float32)
        u = jnp.dot(normed[...], full_gu[1, :, cols], preferred_element_type=jnp.float32)
        hidden[:, cols] = (g / (1.0 + jnp.exp(-g)) * u).astype(jnp.bfloat16)
        return 0

    per_quarter = quarter // TILE
    gathers, lowers = (levels - 1) * chunks, (levels - 1) * pieces

    def filled(g):
        columns = pl.ds(pl.multiple_of((g // 2) * quarter, quarter), quarter)
        taken(full_gu.at[g % 2, pl.ds(0, dim // 2), columns], c_recv.at[g])

    def tiles_by(g):
        return jnp.minimum(2 * (g - 1), per_quarter * ((g + 1) // 2))

    def sent_sum(n):
        return remote(fsum.at[n, peer_rows, :], frecv.at[n], f_sent.at[0], f_recv.at[0], x_peer)

    def lowered(k, zz):
        n = k * levels + zz
        block = full_down.at[k, zz]
        taken(block.at[:, pl.ds(pl.multiple_of((1 - c) * width, width), width)], c_recv.at[chunks + n])
        fsum[n] = jnp.dot(hidden[...], block[...], preferred_element_type=jnp.float32).astype(jnp.bfloat16)
        sent_sum(n).start()

    def settled(v):
        p, zz = side_at(v, pieces)

        @pl.when(p % SPLIT == SPLIT - 1)
        def _():
            lowered(p // SPLIT, zz)

    def steps(first, last):
        def one(i, _):
            line_step(0, i)

            @pl.when(i >= LAG)
            def _():
                from_side(0, i - LAG)

            return 0

        lax.fori_loop(first, last, one, 0)

    loads[0].wait()
    others(lambda zz: out_line(zz, z).start())
    for hh in range(2):
        out_beside(z, hh, c).start()
    loads[5].wait()
    loads[6].wait()
    own(0, chunks)
    for n in range(1, 5):
        loads[n].wait()

    @pl.when(s == 0)
    def _():
        k_buf[pl.ds(0, WINDOW), :] = jnp.zeros((WINDOW, k_buf.shape[1]), k_buf.dtype)
        v_buf[pl.ds(0, WINDOW), :] = jnp.zeros((WINDOW, v_buf.shape[1]), v_buf.dtype)
        d_buf[:, pl.ds(0, WINDOW)] = jnp.full((1, WINDOW), -1, jnp.int32)

    @pl.when(s > 0)
    def _():
        for n in range(3):
            halo(n).wait_recv()

    def out_arrived(t):
        for zz, there in ((z - t, z - t >= 0), (z + t, z + t < levels)):

            @pl.when(there)
            def _(zz=zz):
                out_line(z, zz).wait_recv()
                out_across(zz, y).start()
                out_beside(zz, y, c).start()

    def out_steps(t, _):
        attended(t + 2)
        out_arrived(t)
        return 0

    def attended(n):
        lax.fori_loop(blocks * n // (levels + 2), blocks * (n + 1) // (levels + 2), attention, 0)

    lax.fori_loop(0, 3, lambda n, _: (attended(n), 0)[1], 0)
    lax.fori_loop(1, levels, out_steps, 0)
    steps(0, 1)

    def out_crossed(zz):
        out_across(zz, 1 - y).wait_recv()
        out_beside(zz, 1 - y, c).start()

    others(out_crossed)
    steps(1, 2)
    taken(full_out.at[:, pl.ds(0, dim // 2)], oc_recv.at[0])
    project()
    sent_projection().start()
    steps(2, NORMS_AT)
    loads[9].wait()
    sent_projection().wait()
    norms()
    sent_normed(own_rows).start()
    second = (levels - 2) * chunks
    steps(NORMS_AT, second)
    loads[7].wait()
    loads[8].wait()
    own(1, pieces)
    steps(second, second + LAG + 2)
    sent_normed(own_rows).wait_send()
    sent_normed(peer_rows).wait_recv()
    filled(0)
    filled(1)

    def gated(g, _):
        @pl.when(g + LAG < chunks)
        def _():
            line_step(0, second + g + LAG)

        @pl.when(g + LAG >= chunks)
        def _():
            line_step(1, g + LAG - chunks)

        from_side(0, second + g)
        filled(g)
        lax.fori_loop(tiles_by(g - 1), jnp.where(g == chunks - 1, hid // TILE, tiles_by(g)), hidden_tile, 0)
        return 0

    lax.fori_loop(2, chunks, gated, 0)

    def lowering(u, _):
        line_step(1, u)
        from_side(1, u - LAG)

        @pl.when(u < LAG + 2)
        def _():
            lowered(u - LAG, z)

        settled(u - LAG)
        return 0

    lax.fori_loop(LAG, lowers, lowering, 0)

    def ending(v, _):
        from_side(1, v)
        settled(v)
        return 0

    lax.fori_loop(lowers - LAG, lowers, ending, 0)

    @pl.when(s < count - 1)
    def _():
        for n in range(3):
            halo(n).wait_send()

    def left(block, semaphore):
        remote(block, block, semaphore, semaphore, c_peer).wait_send()

    for n in range(2):
        left(full_out.at[pl.ds(0, out_rows), pl.ds(0, (levels - 1) * out_cols)], o_sent.at[n])
    left(full_out.at[:, pl.ds(0, dim // 2)], o_sent.at[2])
    left(full_gu.at[0, pl.ds(0, (levels - 1) * shard), :], y_sent.at[0])
    left(full_down.at[0, pl.ds(0, levels - 1), pl.ds(0, down_rows), :], y_sent.at[1])
    left(full_gu.at[0], c_sent.at[0])
    left(full_down.at[:, :, :, pl.ds(0, width)], c_sent.at[1])

    def drain(zz, _):
        def one(sent):
            left(full_gu.at[0, pl.ds(0, shard), :], sent.at[0, zz])
            left(full_down.at[0, zz, pl.ds(0, down_rows), :], sent.at[1, zz])

        @pl.when((zz <= z) & (z < levels - 1))
        def _():
            one(z_up)

        @pl.when((zz >= z) & (z > 0))
        def _():
            one(z_dn)

        return 0

    lax.fori_loop(0, levels, drain, 0)
    left(frecv, f_sent.at[0])
    taken(frecv, f_recv.at[0])

    def finish(i, _):
        here = pl.ds(pl.multiple_of(i * FINAL_ROWS, FINAL_ROWS), FINAL_ROWS)
        placed = pl.ds(pl.multiple_of(x * mine + i * FINAL_ROWS, FINAL_ROWS), FINAL_ROWS)
        parts = [
            fsum[k * levels + zz, placed, cc * width : (cc + 1) * width].astype(jnp.float32)
            + frecv[k * levels + zz, here, cc * width : (cc + 1) * width].astype(jnp.float32)
            for zz in range(levels)
            for cc in range(2)
            for k in range(2)
        ]
        ffn_out = jnp.concatenate(parts, axis=1).astype(jnp.bfloat16).astype(jnp.float32)
        out[here, :] = (after[here, :].astype(jnp.float32) + 0.5 * rms_scaled(ffn_out, gain_a[...])).astype(jnp.bfloat16)
        return 0

    lax.fori_loop(0, mine // FINAL_ROWS, finish, 0)


def fused(
    queries, key_rows, value_rows, doc_ids, sink_logits, out_weight,
    residual, gain_mixed, gain_before, gain_after, gate_weight, up_weight, down_weight,
):
    levels = lax.axis_size("sp") // 2
    rows, dim = queries.shape[0], residual.shape[1]
    mine = residual.shape[0]
    hid = gate_weight.shape[1]
    heads = out_weight.shape[0]
    half = down_weight.shape[1] // 2
    vmem, whole = pl.BlockSpec(memory_space=pltpu.VMEM), pl.BlockSpec(memory_space=pl.ANY)
    scalars = pl.BlockSpec(memory_space=pltpu.SMEM)
    bf16, dma = jnp.bfloat16, pltpu.SemaphoreType.DMA
    pieces = 2 * QUARTERS + 2 * SPLIT
    return pl.pallas_call(
        functools.partial(block_kernel, levels),
        out_shape=jax.ShapeDtypeStruct((mine, dim), bf16),
        in_specs=[whole] * 4 + [scalars] + [whole] * 2 + [vmem] * 3 + [whole] * 3,
        out_specs=vmem,
        scratch_shapes=[
            pltpu.VMEM((heads, dim), bf16),
            pltpu.VMEM((2, dim, hid), bf16),
            pltpu.VMEM((2, levels, hid, 2 * half), bf16),
            pltpu.VMEM(queries.shape, bf16),
            pltpu.VMEM((rows + WINDOW, key_rows.shape[1]), bf16),
            pltpu.VMEM((rows + WINDOW, value_rows.shape[1]), bf16),
            pltpu.VMEM((1, rows + WINDOW), jnp.int32),
            pltpu.VMEM(queries.shape, bf16),
            pltpu.VMEM((mine, dim), bf16),
            pltpu.VMEM((rows, dim), bf16),
            pltpu.VMEM((rows, hid), bf16),
            pltpu.VMEM((2 * levels, rows, 2 * half), bf16),
            pltpu.VMEM((2 * levels, mine, 2 * half), bf16),
            dma((10,)),
            dma((3,)),
            dma((3,)),
            dma((3,)),
            dma((levels,)),
            dma((levels,)),
            dma((1,)),
            dma((pieces, levels)),
            dma((2, levels)),
            dma((2, levels)),
            dma((2,)),
            dma((pieces, levels)),
            dma((2,)),
            dma((2 * QUARTERS + 2 * levels,)),
            dma((2,)),
            dma((2,)),
            dma((1,)),
            dma((1,)),
        ],
        compiler_params=pltpu.CompilerParams(collective_id=0, has_side_effects=True, vmem_limit_bytes=67043328),
    )(
        queries, key_rows, value_rows, doc_ids[None], sink_logits, out_weight,
        residual, gain_mixed[None], gain_before[None], gain_after[None], gate_weight, up_weight, down_weight,
    )


def per_device(
    queries,
    key_rows,
    value_rows,
    doc_ids,
    sink_logits,
    out_weight,
    residual,
    gain_mixed,
    gain_before,
    gain_after,
    gate_weight,
    up_weight,
    down_weight,
):
    pairs = lax.axis_size("grp") == 2 and lax.axis_size("tp") == 2
    if pairs and lax.axis_size("sp") % 2 == 0 and lax.axis_size("sp") >= 8:
        return fused(
            queries, key_rows, value_rows, doc_ids, sink_logits, out_weight,
            residual, gain_mixed, gain_before, gain_after, gate_weight, up_weight, down_weight,
        )
    mixed = attend(queries, key_rows, value_rows, doc_ids, sink_logits)
    head_columns = lax.all_gather(out_weight, "sp", axis=1, tiled=True)
    projected = lax.psum_scatter(
        jnp.dot(mixed, head_columns, preferred_element_type=jnp.float32).astype(jnp.bfloat16),
        "tp",
        scatter_dimension=0,
        tiled=True,
    ).astype(jnp.float32)
    projected = stored(projected)
    after = stored(residual.astype(jnp.float32) + rms_scaled(projected, gain_mixed))
    normed = rms_scaled(after, gain_before).astype(jnp.bfloat16)
    full_gate, full_up, full_down = (
        lax.all_gather(gate_weight, "sp", axis=0, tiled=True),
        lax.all_gather(up_weight, "sp", axis=0, tiled=True),
        lax.all_gather(down_weight, "sp", axis=1, tiled=True),
    )
    piece = lax.all_gather(normed, "tp", axis=0, tiled=True)
    gate = jnp.dot(piece, full_gate, preferred_element_type=jnp.float32)
    upward = jnp.dot(piece, full_up, preferred_element_type=jnp.float32)
    hidden = (jax.nn.silu(gate) * upward).astype(jnp.bfloat16)
    ffn_out = stored(
        lax.psum_scatter(
            jnp.dot(hidden, full_down, preferred_element_type=jnp.float32).astype(jnp.bfloat16),
            "tp",
            scatter_dimension=0,
            tiled=True,
        ).astype(jnp.float32)
    )
    return (after + 0.5 * rms_scaled(ffn_out, gain_after)).astype(jnp.bfloat16)


def solution(mesh):
    return jax.shard_map(
        per_device,
        mesh=mesh,
        in_specs=(
            P(("grp", "sp"), "tp"),
            P(("grp", "sp"), "tp"),
            P(("grp", "sp"), "tp"),
            P(("grp", "sp")),
            P("tp"),
            P("tp", "sp"),
            P(("grp", "sp", "tp"), None),
            P(),
            P(),
            P(),
            P("sp", "tp"),
            P("sp", "tp"),
            P("tp", "sp"),
        ),
        out_specs=P(("grp", "sp", "tp"), None),
        check_vma=False,
    )
```

```python
import functools

import jax
import jax.numpy as jnp
from jax import lax
from jax.experimental import pallas as pl
from jax.experimental.pallas import tpu as pltpu
from jax.sharding import PartitionSpec as P

HEAD_DIM = 64
WINDOW = 128


epsilon = 1e-06
masked_value = -1e30


def passed_along(value, axis, steps):
    count = lax.axis_size(axis)
    first, last = (max(0, -steps), min(count, count - steps))
    return lax.ppermute(value, axis, [(source, source + steps) for source in range(first, last)])


def stored(value):
    return lax.optimization_barrier(value.astype(jnp.bfloat16)).astype(jnp.float32)


def rms_scaled(value, gain):
    return value * lax.rsqrt(jnp.mean(value * value, axis=-1, keepdims=True) + epsilon) * gain


def windows(array, blocks):
    first = array[:-WINDOW].reshape((blocks, WINDOW) + array.shape[1:])
    second = array[WINDOW:].reshape((blocks, WINDOW) + array.shape[1:])
    return jnp.concatenate([first, second], axis=1)


def attend(queries, key_rows, value_rows, doc_ids, sink_logits):
    length = queries.shape[0]
    blocks = length // WINDOW
    local_kv = key_rows.shape[1] // HEAD_DIM
    group_size = queries.shape[1] // HEAD_DIM // local_kv
    offset = lax.axis_index("sp") * length
    tail_keys, tail_values, tail_docs = passed_along(
        (key_rows[length - WINDOW :], value_rows[length - WINDOW :], doc_ids[length - WINDOW :]),
        "sp",
        1,
    )
    key_blocks = windows(jnp.concatenate([tail_keys, key_rows], axis=0), blocks).reshape(
        blocks, 2 * WINDOW, local_kv, HEAD_DIM
    )
    value_blocks = windows(jnp.concatenate([tail_values, value_rows], axis=0), blocks).reshape(
        blocks, 2 * WINDOW, local_kv, HEAD_DIM
    )
    key_docs = windows(jnp.concatenate([tail_docs, doc_ids], axis=0), blocks)
    key_places = windows(offset - WINDOW + jnp.arange(length + WINDOW, dtype=jnp.int32), blocks)
    query_places = (offset + jnp.arange(length, dtype=jnp.int32)).reshape(blocks, WINDOW)
    query_docs = doc_ids.reshape(blocks, WINDOW)
    query_blocks = queries.reshape(blocks, WINDOW, local_kv, group_size, HEAD_DIM)
    scores = jnp.einsum(
        "bqhgd,bkhd->bhgqk", query_blocks, key_blocks, preferred_element_type=jnp.float32
    ) * HEAD_DIM ** (-0.5)
    distance = query_places[:, :, None] - key_places[:, None, :]
    valid = (distance >= 0) & (distance < WINDOW) & (key_places[:, None, :] >= 0)
    valid = valid & (query_docs[:, :, None] == key_docs[:, None, :])
    scores = jnp.where(valid[:, None, None], scores, masked_value)
    sinks = sink_logits.reshape(local_kv, group_size)[None, :, :, None]
    top = jnp.maximum(jnp.max(scores, axis=-1), sinks)
    weight = jnp.exp(scores - top[..., None])
    denom = jnp.sum(weight, axis=-1) + jnp.exp(sinks - top)
    summed = jnp.einsum(
        "bhgqk,bkhd->bqhgd",
        weight.astype(jnp.bfloat16),
        value_blocks,
        preferred_element_type=jnp.float32,
    )
    scale = jnp.transpose(denom, (0, 3, 1, 2))[..., None]
    return (summed / scale).reshape(length, queries.shape[1]).astype(jnp.bfloat16)

MESH = pl.DeviceIdType.MESH
QUARTERS = 4
SPLIT = 4
LAG = 2
TILE = 256
STEP_ROWS = 32
FINAL_ROWS = 64
WHOLE = 1
NORMS_AT = 11


def block_kernel(
    levels, queries, keys, values, docs, sinks, wout, resid, gain_m, gain_b, gain_a, gate, up, down, out,
    full_out, full_gu, full_down, q_buf, k_buf, v_buf, d_buf, mixed, after, normed, hidden, fsum, frecv,
    local_sem, halo_send, halo_recv, o_sent, o_recv, oy_recv, oc_recv,
    z_recv, z_up, z_dn, w_recv, w_sent, y_sent, y_recv, c_sent, c_recv, x_send, x_recv, f_sent, f_recv,
):
    y, s, x = lax.axis_index("grp"), lax.axis_index("sp"), lax.axis_index("tp")
    z, c = s // 2, s % 2
    count = 2 * levels
    y_peer, x_peer, c_peer = {"grp": 1 - y}, {"tp": 1 - x}, {"sp": z * 2 + 1 - c}
    above, below = {"sp": jnp.minimum(s + 2, count - 1)}, {"sp": jnp.maximum(s - 2, 0)}
    ahead, behind = {"sp": jnp.minimum(s + 1, count - 1)}, {"sp": jnp.maximum(s - 1, 0)}
    rows, dim, hid = q_buf.shape[0], full_gu.shape[1], full_gu.shape[2]
    mine = after.shape[0]
    blocks = rows // WINDOW
    kv_tiles = k_buf.shape[1] // (2 * HEAD_DIM)
    shard = gate.shape[0]
    half_rows = shard // 2
    out_rows = wout.shape[0] // 2
    out_cols = wout.shape[1]
    down_rows = down.shape[0] // 2
    width = down.shape[1] // 2
    quarter = hid // QUARTERS
    part_rows = down_rows // SPLIT
    chunks, pieces = 2 * QUARTERS, 2 * SPLIT
    own_rows, peer_rows = pl.ds(pl.multiple_of(x * mine, mine), mine), pl.ds(pl.multiple_of((1 - x) * mine, mine), mine)

    barrier = pltpu.get_barrier_semaphore()

    def greet(device):
        pl.semaphore_signal(barrier, inc=1, device_id=device, device_id_type=MESH)

    greet(y_peer)
    greet(x_peer)
    greet(c_peer)

    def greet_line(zz, _):
        @pl.when(zz != z)
        def _():
            greet({"sp": zz * 2 + c})

        return 0

    lax.fori_loop(0, levels, greet_line, 0)

    @pl.when((c == 1) & (z < levels - 1))
    def _():
        greet(ahead)

    @pl.when((c == 0) & (z > 0))
    def _():
        greet(behind)

    def local(source, target, n):
        return pltpu.make_async_copy(source, target, local_sem.at[n])

    shard_rows = pl.ds(pl.multiple_of(s * shard, shard), shard)
    loads = [
        local(wout, full_out.at[:, pl.ds(pl.multiple_of(s * out_cols, out_cols), out_cols)], 0),
        local(keys, k_buf.at[pl.ds(WINDOW, rows), :], 1),
        local(values, v_buf.at[pl.ds(WINDOW, rows), :], 2),
        local(docs, d_buf.at[pl.ds(WINDOW, rows)], 3),
        local(queries, q_buf, 4),
        local(gate, full_gu.at[0, shard_rows, :], 5),
        local(up, full_gu.at[1, shard_rows, :], 6),
        local(down.at[:, pl.ds(0, width)], full_down.at[0, z, :, pl.ds(pl.multiple_of(c * width, width), width)], 7),
        local(down.at[:, pl.ds(width, width)], full_down.at[1, z, :, pl.ds(pl.multiple_of(c * width, width), width)], 8),
        local(resid, after, 9),
    ]
    for load in loads:
        load.start()

    links = jnp.where((c == 1) & (z < levels - 1), 1, 0) + jnp.where((c == 0) & (z > 0), 1, 0)
    pl.semaphore_wait(barrier, 3 + levels - 1 + links)

    def remote(source, target, send, recv, device):
        return pltpu.make_async_remote_copy(
            src_ref=source, dst_ref=target, send_sem=send, recv_sem=recv, device_id=device, device_id_type=MESH
        )

    def halo(n):
        source, target = (
            (keys.at[pl.ds(rows - WINDOW, WINDOW), :], k_buf.at[pl.ds(0, WINDOW), :]),
            (values.at[pl.ds(rows - WINDOW, WINDOW), :], v_buf.at[pl.ds(0, WINDOW), :]),
            (docs.at[pl.ds(rows - WINDOW, WINDOW)], d_buf.at[pl.ds(0, WINDOW)]),
        )[n]
        return remote(source, target, halo_send.at[n], halo_recv.at[n], ahead)

    @pl.when(s < count - 1)
    def _():
        for n in range(3):
            halo(n).start()

    def out_place(zz, cc, hh):
        column = pl.multiple_of((zz * 2 + cc) * out_cols, out_cols)
        return full_out.at[pl.ds(pl.multiple_of(hh * out_rows, out_rows), out_rows), pl.ds(column, out_cols)]

    def out_line(target, source):
        block = out_place(source, c, y)
        return remote(block, block, o_sent.at[0], o_recv.at[source], {"sp": target * 2 + c})

    def out_across(zz, hh):
        block = out_place(zz, c, hh)
        return remote(block, block, o_sent.at[1], oy_recv.at[zz], y_peer)

    def out_beside(zz, hh, cc):
        block = out_place(zz, cc, hh)
        return remote(block, block, o_sent.at[2], oc_recv.at[0], c_peer)

    def others(act):
        def one(zz, _):
            @pl.when(zz != z)
            def _():
                act(zz)

            return 0

        lax.fori_loop(0, levels, one, 0)

    def place(n, zz, cc, hh):
        stage, p = n
        if stage == 0:
            row = pl.multiple_of(((zz * 2 + cc) * 2 + hh) * half_rows, half_rows)
            column = pl.multiple_of((p // 2) * quarter, quarter)
            return full_gu.at[p % 2, pl.ds(row, half_rows), pl.ds(column, quarter)]
        row = pl.multiple_of(hh * down_rows + (p % SPLIT) * part_rows, part_rows)
        return full_down.at[p // SPLIT, zz, pl.ds(row, part_rows), pl.ds(pl.multiple_of(cc * width, width), width)]

    def at(n):
        return n[1] + chunks * n[0]

    def upward(n, zz):
        block = place(n, zz, c, y)
        return remote(block, block, z_up.at[n[0], zz], z_recv.at[at(n), zz], above)

    def downward(n, zz):
        block = place(n, zz, c, y)
        return remote(block, block, z_dn.at[n[0], zz], z_recv.at[at(n), zz], below)

    def across(n, zz, hh):
        block = place(n, zz, c, hh)
        return remote(block, block, y_sent.at[0 if n[0] == 0 else 1 + zz], y_recv.at[at(n), zz], y_peer)

    def whole(p, side, source, device):
        block = place((1, p), source, c, 1 - y)
        return remote(block, block, w_sent.at[side], w_recv.at[p, side], device)

    def whole_from(p, side):
        return whole(p, side, z - 1 + 2 * side, above)

    def beside(n, zz, hh, cc):
        block = place(n, zz, cc, hh)
        group = n[1] if n[0] == 0 else chunks + n[1] // SPLIT * levels + zz
        return remote(block, block, c_sent.at[n[0]], c_recv.at[group], c_peer)

    def own(stage, amount):
        def one(p, _):
            n = (stage, p)

            @pl.when(z < levels - 1)
            def _():
                upward(n, z).start()

            @pl.when(z > 0)
            def _():
                downward(n, z).start()

            for hh in range(2):
                beside(n, z, hh, c).start()

            if stage:

                @pl.when((p < WHOLE) & (z < levels - 1))
                def _():
                    whole(p, 0, z, above).start()

                @pl.when((p < WHOLE) & (z > 0))
                def _():
                    whole(p, 1, z, below).start()

            return 0

        lax.fori_loop(0, amount, one, 0)

    def from_line(n, t):
        low, high = z - t, z + t
        direct = (n[0] == 1) & (t == 1) & (n[1] < WHOLE)

        @pl.when(low >= 0)
        def _():
            upward(n, low).wait_recv()

            @pl.when(z < levels - 1)
            def _():
                upward(n, low).start()

            relayed(n, low, 0, direct)

        @pl.when(high < levels)
        def _():
            downward(n, high).wait_recv()

            @pl.when(z > 0)
            def _():
                downward(n, high).start()

            relayed(n, high, 1, direct)

    def relayed(n, zz, side, direct):
        beside(n, zz, y, c).start()
        if n[0] == 0:
            across(n, zz, y).start()
            return

        @pl.when(jnp.logical_not(direct))
        def _():
            across(n, zz, y).start()

        @pl.when(direct)
        def _():
            whole_from(jnp.minimum(n[1], WHOLE - 1), side).wait_recv()
            beside(n, zz, 1 - y, c).start()

    ends = jnp.minimum(z, levels - 1 - z)

    def side_at(i, amount):
        paired = i < 2 * ends * amount
        rest = i - 2 * ends * amount
        t = jnp.where(paired, i // (2 * amount) + 1, ends + 1 + rest // amount)
        p = jnp.where(paired, (i % (2 * amount)) // 2, rest % amount)
        upper = jnp.where(paired, i % 2 == 1, 2 * z < levels)
        return p, jnp.where(upper, z + t, z - t)

    def from_side(stage, i):
        p, zz = side_at(i, pieces if stage else chunks)
        n = (stage, p)

        def one():
            across(n, zz, 1 - y).wait_recv()
            beside(n, zz, 1 - y, c).start()

        if stage == 0:
            one()
        else:
            near = (zz - z == 1) | (z - zz == 1)
            pl.when(jnp.logical_not(near & (p < WHOLE)))(one)

    def line_step(stage, i):
        amount = pieces if stage else chunks
        from_line((stage, i % amount), i // amount + 1)

    def taken(block, semaphore):
        remote(block, block, semaphore, semaphore, c_peer).wait_recv()

    low_lane = lax.broadcasted_iota(jnp.int32, (1, 2 * HEAD_DIM), 1) < HEAD_DIM

    def attention(b, _):
        here = pl.ds(pl.multiple_of(b * WINDOW, WINDOW), WINDOW)
        span = pl.ds(pl.multiple_of(b * WINDOW, WINDOW), 2 * WINDOW)
        key_docs = d_buf[span][None]
        own_docs = d_buf[pl.ds(pl.multiple_of((b + 1) * WINDOW, WINDOW), WINDOW)][None]
        query_docs = jnp.transpose(jnp.broadcast_to(own_docs, (WINDOW, WINDOW)))
        query_docs = jnp.concatenate([query_docs, query_docs], axis=1)
        query_at = lax.broadcasted_iota(jnp.int32, (WINDOW, 2 * WINDOW), 0)
        key_at = lax.broadcasted_iota(jnp.int32, (WINDOW, 2 * WINDOW), 1)
        valid = (key_at > query_at) & (key_at <= query_at + WINDOW) & (query_docs == key_docs)
        for m in range(kv_tiles):
            lanes = slice(m * 2 * HEAD_DIM, (m + 1) * 2 * HEAD_DIM)
            key_tile = k_buf[span, lanes].astype(jnp.float32)
            value_tile = v_buf[span, lanes].astype(jnp.float32)
            key_turned = pltpu.roll(key_tile, HEAD_DIM, 1)
            value_turned = pltpu.roll(value_tile, HEAD_DIM, 1)
            for e in range(2):
                head = 2 * m + e
                first, second = (key_tile, key_turned) if e == 0 else (key_turned, key_tile)
                key_pair = jnp.where(low_lane, first, second).astype(jnp.bfloat16)
                first, second = (value_tile, value_turned) if e == 0 else (value_turned, value_tile)
                value_pair = jnp.where(low_lane, first, second).astype(jnp.bfloat16)
                columns = slice(head * 2 * HEAD_DIM, (head + 1) * 2 * HEAD_DIM)
                query = q_buf[here, columns].astype(jnp.float32) * HEAD_DIM ** (-0.5)
                stacked = jnp.concatenate(
                    [jnp.where(low_lane, query, 0.0), jnp.where(low_lane, 0.0, query)], axis=0
                ).astype(jnp.bfloat16)
                scores = lax.dot_general(
                    stacked, key_pair, (((1,), (1,)), ((), ())), preferred_element_type=jnp.float32
                )
                results = []
                for g in range(2):
                    sink = sinks[2 * head + g]
                    score = jnp.where(valid, scores[g * WINDOW : (g + 1) * WINDOW], masked_value)
                    top = jnp.maximum(jnp.max(score, axis=1, keepdims=True), sink)
                    weight = jnp.exp(score - top)
                    denom = jnp.sum(weight, axis=1, keepdims=True) + jnp.exp(sink - top)
                    summed = jnp.dot(weight.astype(jnp.bfloat16), value_pair, preferred_element_type=jnp.float32)
                    results.append(summed / denom)
                mixed[here, columns] = jnp.where(low_lane, results[0], results[1]).astype(jnp.bfloat16)
        return 0

    def project():
        def tile(j, _):
            cols = pl.ds(pl.multiple_of(j * TILE, TILE), TILE)
            fsum[j] = jnp.dot(mixed[...], full_out[:, cols], preferred_element_type=jnp.float32).astype(jnp.bfloat16)
            return 0

        lax.fori_loop(0, dim // TILE, tile, 0)

    def sent_projection():
        return remote(fsum.at[:, peer_rows, :], frecv, x_send.at[0], x_recv.at[0], x_peer)

    def sent_normed(where):
        return remote(normed.at[where, :], normed.at[where, :], x_send.at[1], x_recv.at[1], x_peer)

    def norms():
        def tile(i, _):
            here = pl.ds(pl.multiple_of(i * STEP_ROWS, STEP_ROWS), STEP_ROWS)
            placed = pl.ds(pl.multiple_of(x * mine + i * STEP_ROWS, STEP_ROWS), STEP_ROWS)
            parts = [fsum[j, placed, :].astype(jnp.float32) + frecv[j, here, :].astype(jnp.float32) for j in range(dim // TILE)]
            projected = jnp.concatenate(parts, axis=1).astype(jnp.bfloat16).astype(jnp.float32)
            total = (after[here, :].astype(jnp.float32) + rms_scaled(projected, gain_m[...])).astype(jnp.bfloat16)
            after[here, :] = total
            normed[placed, :] = rms_scaled(total.astype(jnp.float32), gain_b[...]).astype(jnp.bfloat16)
            return 0

        lax.fori_loop(0, mine // STEP_ROWS, tile, 0)

    def hidden_tile(j, _):
        cols = pl.ds(pl.multiple_of(j * TILE, TILE), TILE)
        g = jnp.dot(normed[...], full_gu[0, :, cols], preferred_element_type=jnp.float32)
        u = jnp.dot(normed[...], full_gu[1, :, cols], preferred_element_type=jnp.float32)
        hidden[:, cols] = (g / (1.0 + jnp.exp(-g)) * u).astype(jnp.bfloat16)
        return 0

    per_quarter = quarter // TILE
    gathers, lowers = (levels - 1) * chunks, (levels - 1) * pieces

    def filled(g):
        columns = pl.ds(pl.multiple_of((g // 2) * quarter, quarter), quarter)
        taken(full_gu.at[g % 2, pl.ds(0, dim // 2), columns], c_recv.at[g])

    def tiles_by(g):
        return jnp.maximum(per_quarter * (g // 2) - jnp.where(g % 2 == 0, per_quarter // 2, 0), 0)

    def sent_sum(n):
        return remote(fsum.at[n, peer_rows, :], frecv.at[n], f_sent.at[0], f_recv.at[0], x_peer)

    def lowered(k, zz):
        n = k * levels + zz
        block = full_down.at[k, zz]
        taken(block.at[:, pl.ds(pl.multiple_of((1 - c) * width, width), width)], c_recv.at[chunks + n])
        fsum[n] = jnp.dot(hidden[...], block[...], preferred_element_type=jnp.float32).astype(jnp.bfloat16)
        sent_sum(n).start()

    def settled(v):
        p, zz = side_at(v, pieces)

        @pl.when(p % SPLIT == SPLIT - 1)
        def _():
            lowered(p // SPLIT, zz)

    def steps(first, last):
        def one(i, _):
            line_step(0, i)

            @pl.when(i >= LAG)
            def _():
                from_side(0, i - LAG)

            return 0

        lax.fori_loop(first, last, one, 0)

    loads[0].wait()

    def out_sent(t, _):
        for zz, there in ((z - t, z - t >= 0), (z + t, z + t < levels)):

            @pl.when(there)
            def _(zz=zz):
                out_line(zz, z).start()

        return 0

    lax.fori_loop(1, levels, out_sent, 0)
    for hh in range(2):
        out_beside(z, hh, c).start()
    loads[5].wait()
    loads[6].wait()
    own(0, chunks)
    for n in range(1, 5):
        loads[n].wait()

    @pl.when(s == 0)
    def _():
        k_buf[pl.ds(0, WINDOW), :] = jnp.zeros((WINDOW, k_buf.shape[1]), k_buf.dtype)
        v_buf[pl.ds(0, WINDOW), :] = jnp.zeros((WINDOW, v_buf.shape[1]), v_buf.dtype)
        d_buf[pl.ds(0, WINDOW)] = jnp.full((WINDOW,), -1, jnp.int32)

    @pl.when(s > 0)
    def _():
        for n in range(3):
            halo(n).wait_recv()

    def out_arrived(t):
        for zz, there in ((z - t, z - t >= 0), (z + t, z + t < levels)):

            @pl.when(there)
            def _(zz=zz):
                out_line(z, zz).wait_recv()
                out_across(zz, y).start()
                out_beside(zz, y, c).start()

    def out_steps(t, _):
        attended(t + 2)
        out_arrived(t)
        return 0

    def attended(n):
        lax.fori_loop(blocks * n // (levels + 2), blocks * (n + 1) // (levels + 2), attention, 0)

    lax.fori_loop(0, 3, lambda n, _: (attended(n), 0)[1], 0)
    lax.fori_loop(1, levels, out_steps, 0)
    steps(0, 1)

    def out_crossed(zz):
        out_across(zz, 1 - y).wait_recv()
        out_beside(zz, 1 - y, c).start()

    others(out_crossed)
    steps(1, 2)
    taken(full_out.at[:, pl.ds(0, dim // 2)], oc_recv.at[0])
    project()
    sent_projection().start()
    steps(2, NORMS_AT)
    loads[9].wait()
    sent_projection().wait()
    norms()
    sent_normed(own_rows).start()
    second = (levels - 2) * chunks
    steps(NORMS_AT, second)
    loads[7].wait()
    loads[8].wait()
    own(1, pieces)
    steps(second, second + LAG + 2)
    sent_normed(own_rows).wait_send()
    sent_normed(peer_rows).wait_recv()
    filled(0)
    ratio = half_rows * quarter // (part_rows * width)
    behind_by = LAG * ratio

    def gated(g, _):
        @pl.when(g + LAG < chunks)
        def _():
            line_step(0, second + g + LAG)

        @pl.when(g + LAG >= chunks)
        def _():
            for r in range(ratio):
                line_step(1, (g + LAG - chunks) * ratio + r)

        from_side(0, second + g)
        filled(g - 1)
        lax.fori_loop(jnp.where(g == 2, 0, tiles_by(g - 1)), tiles_by(g), hidden_tile, 0)
        return 0

    lax.fori_loop(2, chunks, gated, 0)
    ready = tiles_by(chunks - 1)
    rest = hid // TILE - ready

    def lowering(u, _):
        line_step(1, u)
        v = u - behind_by
        from_side(1, v)

        @pl.when(v == 0)
        def _():
            filled(chunks - 1)

        lax.fori_loop(jnp.minimum(ready + v, hid // TILE), jnp.minimum(ready + v + 1, hid // TILE), hidden_tile, 0)

        @pl.when((v > rest) & (v <= rest + 2))
        def _():
            lowered(v - rest - 1, z)

        @pl.when(v > 0)
        def _():
            settled(v - 1)

        return 0

    lax.fori_loop(behind_by, lowers, lowering, 0)

    def ending(v, _):
        from_side(1, v)
        settled(v - 1)
        return 0

    lax.fori_loop(lowers - behind_by, lowers, ending, 0)
    settled(jnp.int32(lowers - 1))

    @pl.when(s < count - 1)
    def _():
        for n in range(3):
            halo(n).wait_send()

    def left(block, semaphore):
        remote(block, block, semaphore, semaphore, c_peer).wait_send()

    for n in range(2):
        left(full_out.at[pl.ds(0, out_rows), pl.ds(0, (levels - 1) * out_cols)], o_sent.at[n])
    left(full_out.at[:, pl.ds(0, dim // 2)], o_sent.at[2])
    left(full_gu.at[0, pl.ds(0, (levels - 1) * shard), :], y_sent.at[0])
    left(full_gu.at[0], c_sent.at[0])
    left(full_down.at[:, :, :, pl.ds(0, width)], c_sent.at[1])

    def drain(zz, _):
        def one(sent):
            left(full_gu.at[0, pl.ds(0, shard), :], sent.at[0, zz])
            left(full_down.at[0, zz, pl.ds(0, down_rows), :], sent.at[1, zz])

        near = (zz - z == 1) | (z - zz == 1)

        @pl.when(near)
        def _():
            left(full_down.at[0, zz, pl.ds(0, (pieces - WHOLE) * part_rows // 2), :], y_sent.at[1 + zz])

        @pl.when((zz != z) & jnp.logical_not(near))
        def _():
            left(full_down.at[0, zz, pl.ds(0, down_rows), :], y_sent.at[1 + zz])

        @pl.when((zz <= z) & (z < levels - 1))
        def _():
            one(z_up)

        @pl.when((zz >= z) & (z > 0))
        def _():
            one(z_dn)

        return 0

    lax.fori_loop(0, levels, drain, 0)

    @pl.when(z < levels - 1)
    def _():
        left(full_down.at[0, z, pl.ds(0, WHOLE * part_rows // 2), :], w_sent.at[0])

    @pl.when(z > 0)
    def _():
        left(full_down.at[0, z, pl.ds(0, WHOLE * part_rows // 2), :], w_sent.at[1])

    left(frecv, f_sent.at[0])
    taken(frecv, f_recv.at[0])

    def finish(i, _):
        here = pl.ds(pl.multiple_of(i * FINAL_ROWS, FINAL_ROWS), FINAL_ROWS)
        placed = pl.ds(pl.multiple_of(x * mine + i * FINAL_ROWS, FINAL_ROWS), FINAL_ROWS)
        parts = [
            fsum[k * levels + zz, placed, cc * width : (cc + 1) * width].astype(jnp.float32)
            + frecv[k * levels + zz, here, cc * width : (cc + 1) * width].astype(jnp.float32)
            for zz in range(levels)
            for cc in range(2)
            for k in range(2)
        ]
        ffn_out = jnp.concatenate(parts, axis=1).astype(jnp.bfloat16).astype(jnp.float32)
        after[here, :] = (after[here, :].astype(jnp.float32) + 0.5 * rms_scaled(ffn_out, gain_a[...])).astype(jnp.bfloat16)

        @pl.when(i > 0)
        def _():
            written(i - 1).start()

        return 0

    def written(i):
        here = pl.ds(pl.multiple_of(i * FINAL_ROWS, FINAL_ROWS), FINAL_ROWS)
        return pltpu.make_async_copy(after.at[here, :], out.at[here, :], local_sem.at[0])

    lax.fori_loop(0, mine // FINAL_ROWS, finish, 0)
    written(mine // FINAL_ROWS - 1).start()
    pltpu.make_async_copy(after, out, local_sem.at[0]).wait()


def fused(
    queries, key_rows, value_rows, doc_ids, sink_logits, out_weight,
    residual, gain_mixed, gain_before, gain_after, gate_weight, up_weight, down_weight,
):
    levels = lax.axis_size("sp") // 2
    rows, dim = queries.shape[0], residual.shape[1]
    mine = residual.shape[0]
    hid = gate_weight.shape[1]
    heads = out_weight.shape[0]
    half = down_weight.shape[1] // 2
    vmem, whole = pl.BlockSpec(memory_space=pltpu.VMEM), pl.BlockSpec(memory_space=pl.ANY)
    scalars = pl.BlockSpec(memory_space=pltpu.SMEM)
    bf16, dma = jnp.bfloat16, pltpu.SemaphoreType.DMA
    pieces = 2 * QUARTERS + 2 * SPLIT
    return pl.pallas_call(
        functools.partial(block_kernel, levels),
        out_shape=jax.ShapeDtypeStruct((mine, dim), bf16),
        in_specs=[whole] * 4 + [scalars] + [whole] * 2 + [vmem] * 3 + [whole] * 3,
        out_specs=whole,
        scratch_shapes=[
            pltpu.VMEM((heads, dim), bf16),
            pltpu.VMEM((2, dim, hid), bf16),
            pltpu.VMEM((2, levels, hid, 2 * half), bf16),
            pltpu.VMEM(queries.shape, bf16),
            pltpu.VMEM((rows + WINDOW, key_rows.shape[1]), bf16),
            pltpu.VMEM((rows + WINDOW, value_rows.shape[1]), bf16),
            pltpu.VMEM((rows + WINDOW,), jnp.int32),
            pltpu.VMEM(queries.shape, bf16),
            pltpu.VMEM((mine, dim), bf16),
            pltpu.VMEM((rows, dim), bf16),
            pltpu.VMEM((rows, hid), bf16),
            pltpu.VMEM((2 * levels, rows, 2 * half), bf16),
            pltpu.VMEM((2 * levels, mine, 2 * half), bf16),
            dma((10,)),
            dma((3,)),
            dma((3,)),
            dma((3,)),
            dma((levels,)),
            dma((levels,)),
            dma((1,)),
            dma((pieces, levels)),
            dma((2, levels)),
            dma((2, levels)),
            dma((WHOLE, 2)),
            dma((2,)),
            dma((1 + levels,)),
            dma((pieces, levels)),
            dma((2,)),
            dma((2 * QUARTERS + 2 * levels,)),
            dma((2,)),
            dma((2,)),
            dma((1,)),
            dma((1,)),
        ],
        compiler_params=pltpu.CompilerParams(collective_id=0, has_side_effects=True, vmem_limit_bytes=67043328),
    )(
        queries, key_rows, value_rows, doc_ids, sink_logits, out_weight,
        residual, gain_mixed[None], gain_before[None], gain_after[None], gate_weight, up_weight, down_weight,
    )


def per_device(
    queries,
    key_rows,
    value_rows,
    doc_ids,
    sink_logits,
    out_weight,
    residual,
    gain_mixed,
    gain_before,
    gain_after,
    gate_weight,
    up_weight,
    down_weight,
):
    pairs = lax.axis_size("grp") == 2 and lax.axis_size("tp") == 2
    if pairs and lax.axis_size("sp") % 2 == 0 and lax.axis_size("sp") >= 8:
        return fused(
            queries, key_rows, value_rows, doc_ids, sink_logits, out_weight,
            residual, gain_mixed, gain_before, gain_after, gate_weight, up_weight, down_weight,
        )
    mixed = attend(queries, key_rows, value_rows, doc_ids, sink_logits)
    head_columns = lax.all_gather(out_weight, "sp", axis=1, tiled=True)
    projected = lax.psum_scatter(
        jnp.dot(mixed, head_columns, preferred_element_type=jnp.float32).astype(jnp.bfloat16),
        "tp",
        scatter_dimension=0,
        tiled=True,
    ).astype(jnp.float32)
    projected = stored(projected)
    after = stored(residual.astype(jnp.float32) + rms_scaled(projected, gain_mixed))
    normed = rms_scaled(after, gain_before).astype(jnp.bfloat16)
    full_gate, full_up, full_down = (
        lax.all_gather(gate_weight, "sp", axis=0, tiled=True),
        lax.all_gather(up_weight, "sp", axis=0, tiled=True),
        lax.all_gather(down_weight, "sp", axis=1, tiled=True),
    )
    piece = lax.all_gather(normed, "tp", axis=0, tiled=True)
    gate = jnp.dot(piece, full_gate, preferred_element_type=jnp.float32)
    upward = jnp.dot(piece, full_up, preferred_element_type=jnp.float32)
    hidden = (jax.nn.silu(gate) * upward).astype(jnp.bfloat16)
    ffn_out = stored(
        lax.psum_scatter(
            jnp.dot(hidden, full_down, preferred_element_type=jnp.float32).astype(jnp.bfloat16),
            "tp",
            scatter_dimension=0,
            tiled=True,
        ).astype(jnp.float32)
    )
    return (after + 0.5 * rms_scaled(ffn_out, gain_after)).astype(jnp.bfloat16)


def solution(mesh):
    return jax.shard_map(
        per_device,
        mesh=mesh,
        in_specs=(
            P(("grp", "sp"), "tp"),
            P(("grp", "sp"), "tp"),
            P(("grp", "sp"), "tp"),
            P(("grp", "sp")),
            P("tp"),
            P("tp", "sp"),
            P(("grp", "sp", "tp"), None),
            P(),
            P(),
            P(),
            P("sp", "tp"),
            P("sp", "tp"),
            P("tp", "sp"),
        ),
        out_specs=P(("grp", "sp", "tp"), None),
        check_vma=False,
    )
```

```python
import functools

import jax
import jax.numpy as jnp
from jax import lax
from jax.experimental import pallas as pl
from jax.experimental.pallas import tpu as pltpu
from jax.sharding import PartitionSpec as P

HEAD_DIM = 64
WINDOW = 128


epsilon = 1e-06
masked_value = -1e30


def passed_along(value, axis, steps):
    count = lax.axis_size(axis)
    first, last = (max(0, -steps), min(count, count - steps))
    return lax.ppermute(value, axis, [(source, source + steps) for source in range(first, last)])


def stored(value):
    return lax.optimization_barrier(value.astype(jnp.bfloat16)).astype(jnp.float32)


def rms_scaled(value, gain):
    return value * lax.rsqrt(jnp.mean(value * value, axis=-1, keepdims=True) + epsilon) * gain


def windows(array, blocks):
    first = array[:-WINDOW].reshape((blocks, WINDOW) + array.shape[1:])
    second = array[WINDOW:].reshape((blocks, WINDOW) + array.shape[1:])
    return jnp.concatenate([first, second], axis=1)


def attend(queries, key_rows, value_rows, doc_ids, sink_logits):
    length = queries.shape[0]
    blocks = length // WINDOW
    local_kv = key_rows.shape[1] // HEAD_DIM
    group_size = queries.shape[1] // HEAD_DIM // local_kv
    offset = lax.axis_index("sp") * length
    tail_keys, tail_values, tail_docs = passed_along(
        (key_rows[length - WINDOW :], value_rows[length - WINDOW :], doc_ids[length - WINDOW :]),
        "sp",
        1,
    )
    key_blocks = windows(jnp.concatenate([tail_keys, key_rows], axis=0), blocks).reshape(
        blocks, 2 * WINDOW, local_kv, HEAD_DIM
    )
    value_blocks = windows(jnp.concatenate([tail_values, value_rows], axis=0), blocks).reshape(
        blocks, 2 * WINDOW, local_kv, HEAD_DIM
    )
    key_docs = windows(jnp.concatenate([tail_docs, doc_ids], axis=0), blocks)
    key_places = windows(offset - WINDOW + jnp.arange(length + WINDOW, dtype=jnp.int32), blocks)
    query_places = (offset + jnp.arange(length, dtype=jnp.int32)).reshape(blocks, WINDOW)
    query_docs = doc_ids.reshape(blocks, WINDOW)
    query_blocks = queries.reshape(blocks, WINDOW, local_kv, group_size, HEAD_DIM)
    scores = jnp.einsum(
        "bqhgd,bkhd->bhgqk", query_blocks, key_blocks, preferred_element_type=jnp.float32
    ) * HEAD_DIM ** (-0.5)
    distance = query_places[:, :, None] - key_places[:, None, :]
    valid = (distance >= 0) & (distance < WINDOW) & (key_places[:, None, :] >= 0)
    valid = valid & (query_docs[:, :, None] == key_docs[:, None, :])
    scores = jnp.where(valid[:, None, None], scores, masked_value)
    sinks = sink_logits.reshape(local_kv, group_size)[None, :, :, None]
    top = jnp.maximum(jnp.max(scores, axis=-1), sinks)
    weight = jnp.exp(scores - top[..., None])
    denom = jnp.sum(weight, axis=-1) + jnp.exp(sinks - top)
    summed = jnp.einsum(
        "bhgqk,bkhd->bqhgd",
        weight.astype(jnp.bfloat16),
        value_blocks,
        preferred_element_type=jnp.float32,
    )
    scale = jnp.transpose(denom, (0, 3, 1, 2))[..., None]
    return (summed / scale).reshape(length, queries.shape[1]).astype(jnp.bfloat16)

MESH = pl.DeviceIdType.MESH
QUARTERS = 4
HALVES = 2
SPLIT = 4
LAG = 6
TILE = 256
STEP_ROWS = 32
FINAL_ROWS = 64
WHOLE = 1
COPY_PARTS = 6
NORMS_AT = 22


def block_kernel(
    levels, queries, keys, values, docs, sinks, wout, resid, gain_m, gain_b, gain_a, gate, up, down, out,
    full_out, full_gu, full_down, q_buf, k_buf, v_buf, d_buf, mixed, after, normed, hidden, fsum, frecv,
    local_sem, halo_send, halo_recv, o_sent, o_recv, oy_recv, oc_recv,
    z_recv, z_up, z_dn, w_recv, w_sent, y_sent, y_recv, c_sent, c_recv, x_send, x_recv, f_sent, f_recv,
):
    y, s, x = lax.axis_index("grp"), lax.axis_index("sp"), lax.axis_index("tp")
    z, c = s // 2, s % 2
    count = 2 * levels
    y_peer, x_peer, c_peer = {"grp": 1 - y}, {"tp": 1 - x}, {"sp": z * 2 + 1 - c}
    above, below = {"sp": jnp.minimum(s + 2, count - 1)}, {"sp": jnp.maximum(s - 2, 0)}
    ahead, behind = {"sp": jnp.minimum(s + 1, count - 1)}, {"sp": jnp.maximum(s - 1, 0)}
    rows, dim, hid = q_buf.shape[0], full_gu.shape[1], full_gu.shape[2]
    mine = after.shape[0]
    blocks = rows // WINDOW
    kv_tiles = k_buf.shape[1] // (2 * HEAD_DIM)
    shard = gate.shape[0]
    half_rows = shard // 2
    out_rows = wout.shape[0] // 2
    out_cols = wout.shape[1]
    down_rows = down.shape[0] // 2
    width = down.shape[1] // 2
    quarter = hid // QUARTERS
    part_rows = down_rows // SPLIT
    kinds = 2 * QUARTERS
    chunks, pieces = kinds * HALVES, 2 * SPLIT
    chunk_rows = half_rows // HALVES
    own_rows, peer_rows = pl.ds(pl.multiple_of(x * mine, mine), mine), pl.ds(pl.multiple_of((1 - x) * mine, mine), mine)

    barrier = pltpu.get_barrier_semaphore()

    def greet(device):
        pl.semaphore_signal(barrier, inc=1, device_id=device, device_id_type=MESH)

    greet(y_peer)
    greet(x_peer)
    greet(c_peer)

    def greet_line(zz, _):
        @pl.when(zz != z)
        def _():
            greet({"sp": zz * 2 + c})

        return 0

    lax.fori_loop(0, levels, greet_line, 0)

    @pl.when((c == 1) & (z < levels - 1))
    def _():
        greet(ahead)

    @pl.when((c == 0) & (z > 0))
    def _():
        greet(behind)

    def local(source, target, n):
        return pltpu.make_async_copy(source, target, local_sem.at[n])

    shard_rows = pl.ds(pl.multiple_of(s * shard, shard), shard)
    loads = [
        local(wout, full_out.at[:, pl.ds(pl.multiple_of(s * out_cols, out_cols), out_cols)], 0),
        local(keys, k_buf.at[pl.ds(WINDOW, rows), :], 1),
        local(values, v_buf.at[pl.ds(WINDOW, rows), :], 2),
        local(docs, d_buf.at[pl.ds(WINDOW, rows)], 3),
        local(queries, q_buf, 4),
        local(gate, full_gu.at[0, shard_rows, :], 5),
        local(up, full_gu.at[1, shard_rows, :], 6),
        local(down.at[:, pl.ds(0, width)], full_down.at[0, z, :, pl.ds(pl.multiple_of(c * width, width), width)], 7),
        local(down.at[:, pl.ds(width, width)], full_down.at[1, z, :, pl.ds(pl.multiple_of(c * width, width), width)], 8),
        local(resid, after, 9),
    ]
    for load in loads:
        load.start()

    links = jnp.where((c == 1) & (z < levels - 1), 1, 0) + jnp.where((c == 0) & (z > 0), 1, 0)
    pl.semaphore_wait(barrier, 3 + levels - 1 + links)

    def remote(source, target, send, recv, device):
        return pltpu.make_async_remote_copy(
            src_ref=source, dst_ref=target, send_sem=send, recv_sem=recv, device_id=device, device_id_type=MESH
        )

    def halo(n):
        source, target = (
            (keys.at[pl.ds(rows - WINDOW, WINDOW), :], k_buf.at[pl.ds(0, WINDOW), :]),
            (values.at[pl.ds(rows - WINDOW, WINDOW), :], v_buf.at[pl.ds(0, WINDOW), :]),
            (docs.at[pl.ds(rows - WINDOW, WINDOW)], d_buf.at[pl.ds(0, WINDOW)]),
        )[n]
        return remote(source, target, halo_send.at[n], halo_recv.at[n], ahead)

    @pl.when(s < count - 1)
    def _():
        for n in range(3):
            halo(n).start()

    def out_place(zz, cc, hh):
        column = pl.multiple_of((zz * 2 + cc) * out_cols, out_cols)
        return full_out.at[pl.ds(pl.multiple_of(hh * out_rows, out_rows), out_rows), pl.ds(column, out_cols)]

    def out_line(target, source):
        block = out_place(source, c, y)
        return remote(block, block, o_sent.at[0], o_recv.at[source], {"sp": target * 2 + c})

    def out_across(zz, hh):
        block = out_place(zz, c, hh)
        return remote(block, block, o_sent.at[1], oy_recv.at[zz], y_peer)

    def out_beside(zz, hh, cc):
        block = out_place(zz, cc, hh)
        return remote(block, block, o_sent.at[2], oc_recv.at[0], c_peer)

    def others(act):
        def one(zz, _):
            @pl.when(zz != z)
            def _():
                act(zz)

            return 0

        lax.fori_loop(0, levels, one, 0)

    def place(n, zz, cc, hh):
        stage, p = n
        if stage == 0:
            kind = p // HALVES
            row = pl.multiple_of(((zz * 2 + cc) * 2 + hh) * half_rows + p % HALVES * chunk_rows, chunk_rows)
            column = pl.multiple_of((kind // 2) * quarter, quarter)
            return full_gu.at[kind % 2, pl.ds(row, chunk_rows), pl.ds(column, quarter)]
        row = pl.multiple_of(hh * down_rows + (p % SPLIT) * part_rows, part_rows)
        return full_down.at[p // SPLIT, zz, pl.ds(row, part_rows), pl.ds(pl.multiple_of(cc * width, width), width)]

    def at(n):
        return n[1] + chunks * n[0]

    def upward(n, zz):
        block = place(n, zz, c, y)
        return remote(block, block, z_up.at[n[0], zz], z_recv.at[at(n), zz], above)

    def downward(n, zz):
        block = place(n, zz, c, y)
        return remote(block, block, z_dn.at[n[0], zz], z_recv.at[at(n), zz - 1], below)

    def across(n, zz, hh):
        block = place(n, zz, c, hh)
        return remote(block, block, y_sent.at[0 if n[0] == 0 else 1 + zz], y_recv.at[at(n), jnp.where(zz > z, zz - 1, zz)], y_peer)

    def whole(p, side, source, device):
        block = place((1, p), source, c, 1 - y)
        return remote(block, block, w_sent.at[side], w_recv.at[p, side], device)

    def whole_from(p, side):
        return whole(p, side, z - 1 + 2 * side, above)

    def beside(n, zz, hh, cc):
        block = place(n, zz, cc, hh)
        group = n[1] // HALVES if n[0] == 0 else kinds + n[1] // SPLIT * levels + zz
        return remote(block, block, c_sent.at[n[0]], c_recv.at[group], c_peer)

    def own(stage, amount):
        def one(p, _):
            n = (stage, p)

            @pl.when(z < levels - 1)
            def _():
                upward(n, z).start()

            @pl.when(z > 0)
            def _():
                downward(n, z).start()

            for hh in range(2):
                beside(n, z, hh, c).start()

            if stage:

                @pl.when((p < WHOLE) & (z < levels - 1))
                def _():
                    whole(p, 0, z, above).start()

                @pl.when((p < WHOLE) & (z > 0))
                def _():
                    whole(p, 1, z, below).start()

            return 0

        lax.fori_loop(0, amount, one, 0)

    def from_line(n, t):
        low, high = z - t, z + t
        direct = (n[0] == 1) & (t == 1) & (n[1] < WHOLE)

        @pl.when(low >= 0)
        def _():
            upward(n, low).wait_recv()

            @pl.when(z < levels - 1)
            def _():
                upward(n, low).start()

            relayed(n, low, 0, direct)

        @pl.when(high < levels)
        def _():
            downward(n, high).wait_recv()

            @pl.when(z > 0)
            def _():
                downward(n, high).start()

            relayed(n, high, 1, direct)

    def relayed(n, zz, side, direct):
        beside(n, zz, y, c).start()
        if n[0] == 0:
            across(n, zz, y).start()
            return

        @pl.when(jnp.logical_not(direct))
        def _():
            across(n, zz, y).start()

        @pl.when(direct)
        def _():
            whole_from(jnp.minimum(n[1], WHOLE - 1), side).wait_recv()
            beside(n, zz, 1 - y, c).start()

    ends = jnp.minimum(z, levels - 1 - z)

    def side_at(i, amount):
        paired = i < 2 * ends * amount
        rest = i - 2 * ends * amount
        t = jnp.where(paired, i // (2 * amount) + 1, ends + 1 + rest // amount)
        p = jnp.where(paired, (i % (2 * amount)) // 2, rest % amount)
        upper = jnp.where(paired, i % 2 == 1, 2 * z < levels)
        return p, jnp.where(upper, z + t, z - t)

    def from_side(stage, i):
        p, zz = side_at(i, pieces if stage else chunks)
        n = (stage, p)

        def one():
            across(n, zz, 1 - y).wait_recv()
            beside(n, zz, 1 - y, c).start()

        if stage == 0:
            one()
        else:
            near = (zz - z == 1) | (z - zz == 1)
            pl.when(jnp.logical_not(near & (p < WHOLE)))(one)

    def line_step(stage, i):
        amount = pieces if stage else chunks
        from_line((stage, i % amount), i // amount + 1)

    def taken(block, semaphore):
        remote(block, block, semaphore, semaphore, c_peer).wait_recv()

    low_lane = lax.broadcasted_iota(jnp.int32, (1, 2 * HEAD_DIM), 1) < HEAD_DIM

    def attention(b, _):
        here = pl.ds(pl.multiple_of(b * WINDOW, WINDOW), WINDOW)
        span = pl.ds(pl.multiple_of(b * WINDOW, WINDOW), 2 * WINDOW)
        key_docs = d_buf[span][None]
        own_docs = d_buf[pl.ds(pl.multiple_of((b + 1) * WINDOW, WINDOW), WINDOW)][None]
        query_docs = jnp.transpose(jnp.broadcast_to(own_docs, (WINDOW, WINDOW)))
        query_docs = jnp.concatenate([query_docs, query_docs], axis=1)
        query_at = lax.broadcasted_iota(jnp.int32, (WINDOW, 2 * WINDOW), 0)
        key_at = lax.broadcasted_iota(jnp.int32, (WINDOW, 2 * WINDOW), 1)
        valid = (key_at > query_at) & (key_at <= query_at + WINDOW) & (query_docs == key_docs)
        for m in range(kv_tiles):
            lanes = slice(m * 2 * HEAD_DIM, (m + 1) * 2 * HEAD_DIM)
            key_tile = k_buf[span, lanes].astype(jnp.float32)
            value_tile = v_buf[span, lanes].astype(jnp.float32)
            key_turned = pltpu.roll(key_tile, HEAD_DIM, 1)
            value_turned = pltpu.roll(value_tile, HEAD_DIM, 1)
            for e in range(2):
                head = 2 * m + e
                first, second = (key_tile, key_turned) if e == 0 else (key_turned, key_tile)
                key_pair = jnp.where(low_lane, first, second).astype(jnp.bfloat16)
                first, second = (value_tile, value_turned) if e == 0 else (value_turned, value_tile)
                value_pair = jnp.where(low_lane, first, second).astype(jnp.bfloat16)
                columns = slice(head * 2 * HEAD_DIM, (head + 1) * 2 * HEAD_DIM)
                query = q_buf[here, columns].astype(jnp.float32) * HEAD_DIM ** (-0.5)
                stacked = jnp.concatenate(
                    [jnp.where(low_lane, query, 0.0), jnp.where(low_lane, 0.0, query)], axis=0
                ).astype(jnp.bfloat16)
                scores = lax.dot_general(
                    stacked, key_pair, (((1,), (1,)), ((), ())), preferred_element_type=jnp.float32
                )
                results = []
                for g in range(2):
                    sink = sinks[2 * head + g]
                    score = jnp.where(valid, scores[g * WINDOW : (g + 1) * WINDOW], masked_value)
                    top = jnp.maximum(jnp.max(score, axis=1, keepdims=True), sink)
                    weight = jnp.exp(score - top)
                    denom = jnp.sum(weight, axis=1, keepdims=True) + jnp.exp(sink - top)
                    summed = jnp.dot(weight.astype(jnp.bfloat16), value_pair, preferred_element_type=jnp.float32)
                    results.append(summed / denom)
                mixed[here, columns] = jnp.where(low_lane, results[0], results[1]).astype(jnp.bfloat16)
        return 0

    def project():
        def tile(j, _):
            cols = pl.ds(pl.multiple_of(j * TILE, TILE), TILE)
            fsum[j] = jnp.dot(mixed[...], full_out[:, cols], preferred_element_type=jnp.float32).astype(jnp.bfloat16)
            return 0

        lax.fori_loop(0, dim // TILE, tile, 0)

    def sent_projection():
        return remote(fsum.at[:, peer_rows, :], frecv, x_send.at[0], x_recv.at[0], x_peer)

    def sent_normed(where):
        return remote(normed.at[where, :], normed.at[where, :], x_send.at[1], x_recv.at[1], x_peer)

    def norms():
        def tile(i, _):
            here = pl.ds(pl.multiple_of(i * STEP_ROWS, STEP_ROWS), STEP_ROWS)
            placed = pl.ds(pl.multiple_of(x * mine + i * STEP_ROWS, STEP_ROWS), STEP_ROWS)
            parts = [fsum[j, placed, :].astype(jnp.float32) + frecv[j, here, :].astype(jnp.float32) for j in range(dim // TILE)]
            projected = jnp.concatenate(parts, axis=1).astype(jnp.bfloat16).astype(jnp.float32)
            total = (after[here, :].astype(jnp.float32) + rms_scaled(projected, gain_m[...])).astype(jnp.bfloat16)
            after[here, :] = total
            normed[placed, :] = rms_scaled(total.astype(jnp.float32), gain_b[...]).astype(jnp.bfloat16)
            return 0

        lax.fori_loop(0, mine // STEP_ROWS, tile, 0)

    def hidden_tile(j, _):
        cols = pl.ds(pl.multiple_of(j * TILE, TILE), TILE)
        g = jnp.dot(normed[...], full_gu[0, :, cols], preferred_element_type=jnp.float32)
        u = jnp.dot(normed[...], full_gu[1, :, cols], preferred_element_type=jnp.float32)
        hidden[:, cols] = (g / (1.0 + jnp.exp(-g)) * u).astype(jnp.bfloat16)
        return 0

    per_quarter = quarter // TILE
    gathers, lowers = (levels - 1) * chunks, (levels - 1) * pieces

    def filled(g):
        columns = pl.ds(pl.multiple_of((g // 2) * quarter, quarter), quarter)
        taken(full_gu.at[g % 2, pl.ds(0, dim // 2), columns], c_recv.at[g])

    def tiles_at(f):
        most = jnp.minimum(f - 2 * HALVES - 1, per_quarter * (((f + 1) // HALVES - 1) // 2))
        return jnp.where(f < 2 * HALVES + 2, 0, most)

    def sent_sum(n):
        return remote(fsum.at[n, peer_rows, :], frecv.at[n], f_sent.at[0], f_recv.at[0], x_peer)

    def lowered(k, zz):
        n = k * levels + zz
        block = full_down.at[k, zz]
        taken(block.at[:, pl.ds(pl.multiple_of((1 - c) * width, width), width)], c_recv.at[kinds + n])
        fsum[n] = jnp.dot(hidden[...], block[...], preferred_element_type=jnp.float32).astype(jnp.bfloat16)
        sent_sum(n).start()

    def settled(v):
        p, zz = side_at(v, pieces)

        @pl.when(p % SPLIT == SPLIT - 1)
        def _():
            lowered(p // SPLIT, zz)

    def steps(first, last):
        def one(i, _):
            line_step(0, i)

            @pl.when(i >= LAG)
            def _():
                from_side(0, i - LAG)

            return 0

        lax.fori_loop(first, last, one, 0)

    loads[0].wait()

    def out_sent(t, _):
        for zz, there in ((z - t, z - t >= 0), (z + t, z + t < levels)):

            @pl.when(there)
            def _(zz=zz):
                out_line(zz, z).start()

        return 0

    lax.fori_loop(1, levels, out_sent, 0)
    for hh in range(2):
        out_beside(z, hh, c).start()
    loads[5].wait()
    loads[6].wait()
    own(0, chunks)
    for n in range(1, 5):
        loads[n].wait()

    @pl.when(s == 0)
    def _():
        k_buf[pl.ds(0, WINDOW), :] = jnp.zeros((WINDOW, k_buf.shape[1]), k_buf.dtype)
        v_buf[pl.ds(0, WINDOW), :] = jnp.zeros((WINDOW, v_buf.shape[1]), v_buf.dtype)
        d_buf[pl.ds(0, WINDOW)] = jnp.full((WINDOW,), -1, jnp.int32)

    @pl.when(s > 0)
    def _():
        for n in range(3):
            halo(n).wait_recv()

    def out_arrived(t):
        for zz, there in ((z - t, z - t >= 0), (z + t, z + t < levels)):

            @pl.when(there)
            def _(zz=zz):
                out_line(z, zz).wait_recv()
                out_across(zz, y).start()
                out_beside(zz, y, c).start()

    def out_steps(t, _):
        attended(t + 2)
        out_arrived(t)
        return 0

    def attended(n):
        lax.fori_loop(blocks * n // (levels + 2), blocks * (n + 1) // (levels + 2), attention, 0)

    lax.fori_loop(0, 3, lambda n, _: (attended(n), 0)[1], 0)
    lax.fori_loop(1, 2, out_steps, 0)
    steps(0, 1)
    lax.fori_loop(2, levels, out_steps, 0)
    steps(1, 4)

    def out_crossed(zz):
        out_across(zz, 1 - y).wait_recv()
        out_beside(zz, 1 - y, c).start()

    others(out_crossed)
    steps(4, 6)
    taken(full_out.at[:, pl.ds(0, dim // 2)], oc_recv.at[0])
    project()
    sent_projection().start()
    steps(6, NORMS_AT)
    loads[9].wait()
    sent_projection().wait()
    norms()
    sent_normed(own_rows).start()
    second = (levels - 2) * chunks
    steps(NORMS_AT, second)
    loads[7].wait()
    loads[8].wait()
    own(1, pieces)
    steps(second, second + LAG + 2 * HALVES)
    filled(0)
    def gated(f, _):
        g = f // HALVES

        @pl.when(f + LAG < chunks)
        def _():
            line_step(0, second + f + LAG)

        @pl.when(f + LAG >= chunks)
        def _():
            line_step(1, f + LAG - chunks)

        from_side(0, second + f)

        @pl.when(f % HALVES == HALVES - 1)
        def _():
            filled(g - 1)

        @pl.when(f == 2 * HALVES + 2)
        def _():
            sent_normed(own_rows).wait_send()
            sent_normed(peer_rows).wait_recv()

        lax.fori_loop(tiles_at(f - 1), tiles_at(f), hidden_tile, 0)
        return 0

    lax.fori_loop(2 * HALVES, chunks, gated, 0)
    ready = tiles_at(chunks - 1)
    rest = hid // TILE - ready

    def lowering(u, _):
        line_step(1, u)
        v = u - LAG
        from_side(1, v)

        @pl.when(v == 0)
        def _():
            filled(kinds - 1)

        lax.fori_loop(jnp.minimum(ready + v, hid // TILE), jnp.minimum(ready + v + 1, hid // TILE), hidden_tile, 0)

        @pl.when((v > rest) & (v <= rest + 2))
        def _():
            lowered(v - rest - 1, z)

        @pl.when(v > 0)
        def _():
            settled(v - 1)

        return 0

    lax.fori_loop(LAG, lowers, lowering, 0)

    def ending(v, _):
        from_side(1, v)
        settled(v - 1)
        return 0

    lax.fori_loop(lowers - LAG, lowers, ending, 0)
    settled(jnp.int32(lowers - 1))

    @pl.when(s < count - 1)
    def _():
        for n in range(3):
            halo(n).wait_send()

    def left(block, semaphore):
        remote(block, block, semaphore, semaphore, c_peer).wait_send()

    for n in range(2):
        left(full_out.at[pl.ds(0, out_rows), pl.ds(0, (levels - 1) * out_cols)], o_sent.at[n])
    left(full_out.at[:, pl.ds(0, dim // 2)], o_sent.at[2])
    left(full_gu.at[0, pl.ds(0, (levels - 1) * shard), :], y_sent.at[0])
    left(full_gu.at[0], c_sent.at[0])
    left(full_down.at[:, :, :, pl.ds(0, width)], c_sent.at[1])

    def drain(zz, _):
        def one(sent):
            left(full_gu.at[0, pl.ds(0, shard), :], sent.at[0, zz])
            left(full_down.at[0, zz, pl.ds(0, down_rows), :], sent.at[1, zz])

        near = (zz - z == 1) | (z - zz == 1)

        @pl.when(near)
        def _():
            left(full_down.at[0, zz, pl.ds(0, (pieces - WHOLE) * part_rows // 2), :], y_sent.at[1 + zz])

        @pl.when((zz != z) & jnp.logical_not(near))
        def _():
            left(full_down.at[0, zz, pl.ds(0, down_rows), :], y_sent.at[1 + zz])

        @pl.when((zz <= z) & (z < levels - 1))
        def _():
            one(z_up)

        @pl.when((zz >= z) & (z > 0))
        def _():
            one(z_dn)

        return 0

    lax.fori_loop(0, levels, drain, 0)

    @pl.when(z < levels - 1)
    def _():
        left(full_down.at[0, z, pl.ds(0, WHOLE * part_rows // 2), :], w_sent.at[0])

    @pl.when(z > 0)
    def _():
        left(full_down.at[0, z, pl.ds(0, WHOLE * part_rows // 2), :], w_sent.at[1])

    left(frecv, f_sent.at[0])
    taken(frecv, f_recv.at[0])

    def finish(i, _):
        here = pl.ds(pl.multiple_of(i * FINAL_ROWS, FINAL_ROWS), FINAL_ROWS)
        placed = pl.ds(pl.multiple_of(x * mine + i * FINAL_ROWS, FINAL_ROWS), FINAL_ROWS)
        parts = [
            fsum[k * levels + zz, placed, cc * width : (cc + 1) * width].astype(jnp.float32)
            + frecv[k * levels + zz, here, cc * width : (cc + 1) * width].astype(jnp.float32)
            for zz in range(levels)
            for cc in range(2)
            for k in range(2)
        ]
        ffn_out = jnp.concatenate(parts, axis=1).astype(jnp.bfloat16).astype(jnp.float32)
        after[here, :] = (after[here, :].astype(jnp.float32) + 0.5 * rms_scaled(ffn_out, gain_a[...])).astype(jnp.bfloat16)

        @pl.when(i > 0)
        def _():
            written(i - 1).start()

        return 0

    def written(i):
        here = pl.ds(pl.multiple_of(i * FINAL_ROWS, FINAL_ROWS), FINAL_ROWS)
        return pltpu.make_async_copy(after.at[here, :], out.at[here, :], local_sem.at[0])

    lax.fori_loop(0, mine // FINAL_ROWS, finish, 0)
    written(mine // FINAL_ROWS - 1).start()
    pltpu.make_async_copy(after, out, local_sem.at[0]).wait()


def copy_kernel(source, target, held, arrived, left):
    parts = held.shape[0]
    rows = held.shape[1]

    def taken(n):
        return pltpu.make_async_copy(source.at[pl.ds(n * rows, rows), :], held.at[n], arrived.at[n])

    def given(n):
        return pltpu.make_async_copy(held.at[n], target.at[pl.ds(n * rows, rows), :], left.at[n])

    for n in range(parts):
        taken(n).start()
    for n in range(parts):
        taken(n).wait()
        given(n).start()
    for n in range(parts):
        given(n).wait()


def copied(array):
    parts, whole = COPY_PARTS, pl.BlockSpec(memory_space=pl.ANY)
    return pl.pallas_call(
        copy_kernel,
        out_shape=jax.ShapeDtypeStruct(array.shape, array.dtype),
        in_specs=[whole],
        out_specs=whole,
        scratch_shapes=[
            pltpu.VMEM((parts, array.shape[0] // parts, array.shape[1]), array.dtype),
            pltpu.SemaphoreType.DMA((parts,)),
            pltpu.SemaphoreType.DMA((parts,)),
        ],
    )(array)


def fused(
    queries, key_rows, value_rows, doc_ids, sink_logits, out_weight,
    residual, gain_mixed, gain_before, gain_after, gate_weight, up_weight, down_weight,
):
    levels = lax.axis_size("sp") // 2
    rows, dim = queries.shape[0], residual.shape[1]
    mine = residual.shape[0]
    hid = gate_weight.shape[1]
    heads = out_weight.shape[0]
    half = down_weight.shape[1] // 2
    vmem, whole = pl.BlockSpec(memory_space=pltpu.VMEM), pl.BlockSpec(memory_space=pl.ANY)
    scalars = pl.BlockSpec(memory_space=pltpu.SMEM)
    bf16, dma = jnp.bfloat16, pltpu.SemaphoreType.DMA
    pieces = 2 * QUARTERS * HALVES + 2 * SPLIT
    return pl.pallas_call(
        functools.partial(block_kernel, levels),
        out_shape=jax.ShapeDtypeStruct((mine, dim), bf16),
        in_specs=[whole] * 4 + [scalars] + [whole] * 2 + [vmem] * 3 + [whole] * 3,
        out_specs=whole,
        scratch_shapes=[
            pltpu.VMEM((heads, dim), bf16),
            pltpu.VMEM((2, dim, hid), bf16),
            pltpu.VMEM((2, levels, hid, 2 * half), bf16),
            pltpu.VMEM(queries.shape, bf16),
            pltpu.VMEM((rows + WINDOW, key_rows.shape[1]), bf16),
            pltpu.VMEM((rows + WINDOW, value_rows.shape[1]), bf16),
            pltpu.VMEM((rows + WINDOW,), jnp.int32),
            pltpu.VMEM(queries.shape, bf16),
            pltpu.VMEM((mine, dim), bf16),
            pltpu.VMEM((rows, dim), bf16),
            pltpu.VMEM((rows, hid), bf16),
            pltpu.VMEM((2 * levels, rows, 2 * half), bf16),
            pltpu.VMEM((2 * levels, mine, 2 * half), bf16),
            dma((10,)),
            dma((3,)),
            dma((3,)),
            dma((3,)),
            dma((levels,)),
            dma((levels,)),
            dma((1,)),
            dma((pieces, levels - 1)),
            dma((2, levels)),
            dma((2, levels)),
            dma((WHOLE, 2)),
            dma((2,)),
            dma((1 + levels,)),
            dma((pieces, levels - 1)),
            dma((2,)),
            dma((2 * QUARTERS + 2 * levels,)),
            dma((2,)),
            dma((2,)),
            dma((1,)),
            dma((1,)),
        ],
        compiler_params=pltpu.CompilerParams(collective_id=0, has_side_effects=True, vmem_limit_bytes=67043328),
    )(
        queries, key_rows, value_rows, doc_ids, sink_logits, out_weight,
        residual, gain_mixed[None], gain_before[None], gain_after[None], gate_weight, up_weight, down_weight,
    )


def per_device(
    queries,
    key_rows,
    value_rows,
    doc_ids,
    sink_logits,
    out_weight,
    residual,
    gain_mixed,
    gain_before,
    gain_after,
    gate_weight,
    up_weight,
    down_weight,
):
    pairs = lax.axis_size("grp") == 2 and lax.axis_size("tp") == 2
    if pairs and lax.axis_size("sp") % 2 == 0 and lax.axis_size("sp") >= 8:
        return copied(
            fused(
                queries, key_rows, value_rows, doc_ids, sink_logits, out_weight,
                residual, gain_mixed, gain_before, gain_after, gate_weight, up_weight, down_weight,
            )
        )
    mixed = attend(queries, key_rows, value_rows, doc_ids, sink_logits)
    head_columns = lax.all_gather(out_weight, "sp", axis=1, tiled=True)
    projected = lax.psum_scatter(
        jnp.dot(mixed, head_columns, preferred_element_type=jnp.float32).astype(jnp.bfloat16),
        "tp",
        scatter_dimension=0,
        tiled=True,
    ).astype(jnp.float32)
    projected = stored(projected)
    after = stored(residual.astype(jnp.float32) + rms_scaled(projected, gain_mixed))
    normed = rms_scaled(after, gain_before).astype(jnp.bfloat16)
    full_gate, full_up, full_down = (
        lax.all_gather(gate_weight, "sp", axis=0, tiled=True),
        lax.all_gather(up_weight, "sp", axis=0, tiled=True),
        lax.all_gather(down_weight, "sp", axis=1, tiled=True),
    )
    piece = lax.all_gather(normed, "tp", axis=0, tiled=True)
    gate = jnp.dot(piece, full_gate, preferred_element_type=jnp.float32)
    upward = jnp.dot(piece, full_up, preferred_element_type=jnp.float32)
    hidden = (jax.nn.silu(gate) * upward).astype(jnp.bfloat16)
    ffn_out = stored(
        lax.psum_scatter(
            jnp.dot(hidden, full_down, preferred_element_type=jnp.float32).astype(jnp.bfloat16),
            "tp",
            scatter_dimension=0,
            tiled=True,
        ).astype(jnp.float32)
    )
    return (after + 0.5 * rms_scaled(ffn_out, gain_after)).astype(jnp.bfloat16)


def solution(mesh):
    return jax.shard_map(
        per_device,
        mesh=mesh,
        in_specs=(
            P(("grp", "sp"), "tp"),
            P(("grp", "sp"), "tp"),
            P(("grp", "sp"), "tp"),
            P(("grp", "sp")),
            P("tp"),
            P("tp", "sp"),
            P(("grp", "sp", "tp"), None),
            P(),
            P(),
            P(),
            P("sp", "tp"),
            P("sp", "tp"),
            P("tp", "sp"),
        ),
        out_specs=P(("grp", "sp", "tp"), None),
        check_vma=False,
    )
```
